512 devices in a mesh: sp: 32 (over z, core), tp: 16 (over y, x).
Axes of the slice: x: 4, y: 4, z: 16, core: 2. Of those that a mesh axis runs over, the one named last changes fastest.
Arguments:
- wide_queries: bfloat16 [2048, 2560], P('sp', 'tp'), may hold values from -512 to 512
- narrow_queries: bfloat16 [2048, 1536], P('sp', 'tp'), may hold values from -512 to 512
- kv_latent: bfloat16 [2048, 512], P('sp'), may hold values from -6 to 6
- rope_key: bfloat16 [2048, 32], P('sp'), may hold values from -4 to 4
- latent_gain: float32 [512], replicated, may hold values from 0.1 to 1.9
- wide_kv_weight: bfloat16 [512, 4096], P(None, 'tp'), may hold values from -0.25 to 0.25
- narrow_kv_weight: bfloat16 [512, 2048], P(None, 'tp'), may hold values from -0.25 to 0.25
- wide_out_weight: bfloat16 [2048, 2048], P('tp'), may hold values from -0.4375 to 0.4375
- narrow_out_weight: bfloat16 [1024, 2048], P('tp'), may hold values from -0.4375 to 0.4375
- residual: bfloat16 [2048, 2048], P('sp'), may hold values from -6 to 6
- norm_gain: float32 [2048], replicated, may hold values from 0.1 to 1.9
- route_ids: int32 [2048, 2], P('sp'), may hold values from 0 to 63, all different within a row; in each aligned block of 64 rows (0 to 63, 64 to 127, ...) at most 3 rows name the same one
- route_weights: float32 [2048, 2], P('sp'), may hold values from 0.3 to 1.3
- expert_gate: bfloat16 [64, 2048, 1024], P('sp', None, 'tp'), may hold values from -0.125 to 0.125
- expert_up: bfloat16 [64, 2048, 1024], P('sp', None, 'tp'), may hold values from -0.125 to 0.125
- expert_down: bfloat16 [64, 1024, 2048], P('sp', 'tp'), may hold values from -0.1875 to 0.1875
- shared_gate: bfloat16 [2048, 1024], P(None, 'tp'), may hold values from -0.125 to 0.125
- shared_up: bfloat16 [2048, 1024], P(None, 'tp'), may hold values from -0.125 to 0.125
- shared_down: bfloat16 [1024, 2048], P('tp'), may hold values from -0.1875 to 0.1875
Outputs:
- mixed_out: bfloat16 [2048, 2048], P('sp', 'tp')
The draws below stay inside these ranges and needn't reach their ends.
Inputs may be any that keep to these rules, and one draw needn't show every extreme that they name: `route_ids`: in the rows of one index of sp (aligned blocks of 64 rows) no expert is named by more than 3 rows, and some expert by exactly that many; each row names 2 different experts.
All inputs are finite; a program needn't handle non-finite values.
Results may differ from the reference program's by a relative error of at most 0.018.
Values may be sent and summed in bfloat16 or wider, within the bound.
A program may use at most 64 MiB of HBM per device.

```python
import math
import jax
import jax.numpy as jnp
import numpy as np
from jax import lax

D_MODEL = 2048
WIDE_HEADS = 16
NARROW_HEADS = 16
WIDE_NOPE = 128
WIDE_VALUE = 128
NARROW_NOPE = 64
NARROW_VALUE = 64
ROPE_DIM = 32
LATENT = 512
EXPERT_FF = 1024
TOP_K = 2
TOK_DEV = 64
TOKENS = 2048
EXPERTS = 64
CAPACITY = 3
N_SP = 32
N_TP = 16


def queries_for(key, head_count, nope_width, salt):
    full_width = nope_width + ROPE_DIM
    base = 2.0 * jax.random.normal(jax.random.fold_in(key, salt), (TOKENS, head_count, full_width), jnp.float32)
    base = jnp.clip(base, -12.0, 12.0)
    return base.reshape(TOKENS, head_count * full_width).astype(jnp.bfloat16)


def draw_wide_queries(key, part):
    return queries_for(key, WIDE_HEADS, WIDE_NOPE, 31)


def draw_narrow_queries(key, part):
    return queries_for(key, NARROW_HEADS, NARROW_NOPE, 32)


def draw_rope_key(key, part):
    base = jnp.clip(jax.random.normal(jax.random.fold_in(key, 21), (TOKENS, ROPE_DIM), jnp.float32), -4.0, 4.0)
    return base.astype(jnp.bfloat16)


def shard_levels(rng, shape, split, least, top_value):
    loudness, own = 1.0, jax.random.fold_in(rng, 6)
    for axis_at, blocks in split:
        draws = jnp.exp(jax.random.uniform(jax.random.fold_in(own, axis_at), (blocks,), jnp.float32, least / len(split), top_value / len(split)))
        loudness = loudness * jnp.repeat(draws, shape[axis_at] // blocks).reshape([-1 if axis == axis_at else 1 for axis in range(len(shape))])
    return loudness


def routed_block(own_key, own, number, rows, count, top, most, lean):
    ranking = jax.random.permutation(own_key, count)
    packed, usual = portions_of(count, rows * top, most, lean, True), portions_of(count, rows * top, most, lean, False)
    places = jnp.arange(count)

    def named(lengths, turn):
        used = int((lengths > 0).sum())
        fixed = max(1, used // 4)
        moved = fixed + (places - fixed + turn * (used - fixed)) % max(1, count - fixed)
        return jnp.zeros((count,), jnp.int32).at[ranking[jnp.where(places < fixed, places, moved)]].set(jnp.asarray(lengths, jnp.int32))

    lengths = jnp.where(number % 4 == 0, named(packed, number // 4), named(usual, number - number // 4 - 1))
    mixed = jax.random.permutation(jax.random.fold_in(own, 3), count)
    source_of, sink = mixed[0:count // 2 * 2:2], mixed[1:count // 2 * 2:2]
    room = jnp.minimum(lengths[source_of] - 1, most - lengths[sink]) // 2
    room = jnp.where((source_of == ranking[0]) | (sink == ranking[0]) | (lengths[sink] == 0), 0, jnp.maximum(room, 0))
    moved = jax.random.randint(jax.random.fold_in(own, 4), (count // 2,), 0, 1 << 20) % (room + 1)
    lengths = lengths.at[source_of].add(-moved).at[sink].add(moved)
    members = jnp.searchsorted(jnp.cumsum(lengths), jnp.arange(rows * top), side="right").astype(jnp.int32)
    table = members.reshape(top, rows).T
    table = table[jax.random.permutation(jax.random.fold_in(own, 1), rows)]
    turn = jax.random.randint(jax.random.fold_in(own, 2), (rows, 1), 0, top)
    return jnp.take_along_axis(table, (jnp.arange(top)[None, :] + turn) % top, axis=1)


def portions_of(count, total, reach, lean, full):
    portions = [(1 << 20) // math.isqrt(rank ** lean) + 1 for rank in range(1, count + 1)]
    largest = reach if full else min(reach, max(-(-total // count), total * portions[0] // sum(portions)))
    least = 1 if total - largest >= count - 1 else 0
    given, rest = [largest] + [least] * (count - 1), total - largest - least * (count - 1)
    while rest > 0:
        free = [i for i in range(1, count) if given[i] < largest] or [i for i in range(1, count) if given[i] < reach]
        mass, remaining = sum([portions[i] for i in free]), rest
        for i in free:
            addition = min(reach - given[i], max(1, remaining * portions[i] // mass), rest)
            given[i] = given[i] + addition
            rest = rest - addition
    return np.array(given)


def normal_values(rng, dims, scale, reach, split=(), kind=jnp.bfloat16):
    entries = scale * jax.random.normal(rng, dims, jnp.float32)
    if split:
        entries = entries * shard_levels(rng, dims, split, -0.22, 0.18)
    return jnp.clip(entries, -reach, reach).astype(kind)


def setup_inputs(seed: int = 0) -> dict:
    key_list = jax.random.split(jax.random.key(seed), 20)
    wide_queries = draw_wide_queries(jax.random.fold_in(key_list[19], 71), 0)
    narrow_queries = draw_narrow_queries(jax.random.fold_in(key_list[19], 71), 0)
    kv_latent = normal_values(key_list[2], (TOKENS, LATENT), 1.0, 6.0, ((0, 32),))
    rope_key = draw_rope_key(jax.random.fold_in(key_list[19], 71), 0)
    latent_gain = jnp.clip(1.0 + 0.18 * jax.random.normal(key_list[4], (LATENT,), jnp.float32), 0.1, 1.9)
    wide_kv_weight = normal_values(key_list[5], (LATENT, WIDE_HEADS * (WIDE_NOPE + WIDE_VALUE)), LATENT ** -0.5, 0.25, ((1, 16),))
    narrow_kv_weight = normal_values(key_list[6], (LATENT, NARROW_HEADS * (NARROW_NOPE + NARROW_VALUE)), LATENT ** -0.5, 0.25, ((1, 16),))
    wide_out_weight = normal_values(key_list[7], (WIDE_HEADS * WIDE_VALUE, D_MODEL), ((WIDE_HEADS * WIDE_VALUE + NARROW_HEADS * NARROW_VALUE) // 16) ** -0.5, 0.4375, ((0, 16),))
    narrow_out_weight = normal_values(key_list[8], (NARROW_HEADS * NARROW_VALUE, D_MODEL), ((WIDE_HEADS * WIDE_VALUE + NARROW_HEADS * NARROW_VALUE) // 16) ** -0.5, 0.4375, ((0, 16),))
    residual = normal_values(key_list[9], (TOKENS, D_MODEL), 1.0, 6.0, ((0, 32),))
    norm_gain = jnp.clip(1.0 + 0.18 * jax.random.normal(key_list[10], (D_MODEL,), jnp.float32), 0.1, 1.9)
    route_ids_keys = jax.random.split(jax.random.fold_in(key_list[11], 1), TOKENS // TOK_DEV)
    route_ids_turns = jax.random.permutation(jax.random.fold_in(key_list[11], 3), TOKENS // TOK_DEV)
    route_ids = jax.vmap(lambda own, number: routed_block(jax.random.fold_in(key_list[11], 2), own, number, TOK_DEV, EXPERTS, TOP_K, CAPACITY, 1))(route_ids_keys, route_ids_turns).reshape((TOKENS, TOP_K))
    route_weights = jnp.clip(0.3 + 0.99999994 * jax.random.uniform(key_list[12], (TOKENS, TOP_K), jnp.float32) ** shard_levels(key_list[12], (TOKENS, TOP_K), ((0, 32),), -0.2, 0.2), 0.3, 1.3)
    expert_gate = normal_values(key_list[13], (EXPERTS, D_MODEL, EXPERT_FF), D_MODEL ** -0.5, 0.125, ((0, 32), (2, 16)))
    expert_up = normal_values(key_list[14], (EXPERTS, D_MODEL, EXPERT_FF), D_MODEL ** -0.5, 0.125, ((0, 32), (2, 16)))
    expert_down = normal_values(key_list[15], (EXPERTS, EXPERT_FF, D_MODEL), EXPERT_FF ** -0.5, 0.1875, ((0, 32), (1, 16)))
    shared_gate = normal_values(key_list[16], (D_MODEL, EXPERT_FF), D_MODEL ** -0.5, 0.125, ((1, 16),))
    shared_up = normal_values(key_list[17], (D_MODEL, EXPERT_FF), D_MODEL ** -0.5, 0.125, ((1, 16),))
    shared_down = normal_values(key_list[18], (EXPERT_FF, D_MODEL), EXPERT_FF ** -0.5, 0.1875, ((0, 16),))
    return dict(wide_queries=wide_queries, narrow_queries=narrow_queries, kv_latent=kv_latent, rope_key=rope_key, latent_gain=latent_gain, wide_kv_weight=wide_kv_weight, narrow_kv_weight=narrow_kv_weight, wide_out_weight=wide_out_weight, narrow_out_weight=narrow_out_weight, residual=residual, norm_gain=norm_gain, route_ids=route_ids, route_weights=route_weights, expert_gate=expert_gate, expert_up=expert_up, expert_down=expert_down, shared_gate=shared_gate, shared_up=shared_up, shared_down=shared_down)


THETA = 10000.0
EPS = 1e-06

def stored(values):
    return lax.optimization_barrier(values.astype(jnp.bfloat16))

def rotate(values, positions):
    half_width = values.shape[-1] // 2
    frequency = THETA ** (-2.0 * jnp.arange(half_width, dtype=jnp.float32) / values.shape[-1])
    angles = positions.astype(jnp.float32)[:, None] * frequency[None, :]
    if values.ndim == 3:
        angles = angles[:, None, :]
    cosine = jnp.cos(angles)
    sine_part = jnp.sin(angles)
    as_float = values.astype(jnp.float32)
    first_half = as_float[..., :half_width]
    second_half = as_float[..., half_width:]
    return stored(jnp.concatenate([first_half * cosine - second_half * sine_part, second_half * cosine + first_half * sine_part], axis=-1))

def rms_scale(values, gain):
    as_float = values.astype(jnp.float32)
    scaled = as_float * lax.rsqrt(lax.optimization_barrier(jnp.mean(as_float * as_float, axis=-1, keepdims=True)) + EPS)
    return stored(scaled * gain)

def attend(queries, nope_width, key_nope, key_rot, values):
    token_count = queries.shape[0]
    scale = queries.shape[-1] ** (-0.5)
    query_nope = queries[..., :nope_width].astype(jnp.float32)
    query_rope = queries[..., nope_width:].astype(jnp.float32)
    keys_float = key_nope.astype(jnp.float32)
    rot_float = key_rot.astype(jnp.float32)
    values_float = values.astype(jnp.float32)
    key_pos = jnp.arange(token_count, dtype=jnp.int32)

    def one_block(block_index):
        first_row = (block_index * TOK_DEV).astype(jnp.int32)
        block_nope = lax.dynamic_slice_in_dim(query_nope, first_row, TOK_DEV, 0)
        block_rope = lax.dynamic_slice_in_dim(query_rope, first_row, TOK_DEV, 0)
        scores = jnp.einsum('qhd,khd->hqk', block_nope, keys_float)
        scores = (scores + jnp.einsum('qhr,kr->hqk', block_rope, rot_float)) * scale
        query_pos = first_row + jnp.arange(TOK_DEV, dtype=jnp.int32)
        allowed = (query_pos[:, None] >= key_pos[None, :])[None]
        scores = jnp.where(allowed, scores, -jnp.inf)
        row_peak = lax.optimization_barrier(jnp.max(scores, axis=-1, keepdims=True))
        expo = jnp.exp(scores - row_peak)
        row_total = lax.optimization_barrier(jnp.sum(expo, axis=-1))
        probs = stored(expo).astype(jnp.float32)
        mixed = jnp.einsum('hqk,khv->qhv', probs, values_float)
        return stored(mixed / row_total.T[:, :, None])
    blocks = lax.map(one_block, jnp.arange(token_count // TOK_DEV, dtype=jnp.int32))
    return blocks.reshape(token_count, queries.shape[1], values.shape[-1])

def reference(wide_queries, narrow_queries, kv_latent, rope_key, latent_gain, wide_kv_weight, narrow_kv_weight, wide_out_weight, narrow_out_weight, residual, norm_gain, route_ids, route_weights, expert_gate, expert_up, expert_down, shared_gate, shared_up, shared_down):
    token_count = residual.shape[0]
    positions = jnp.arange(token_count, dtype=jnp.int32)
    wide_q = wide_queries.reshape(token_count, WIDE_HEADS, WIDE_NOPE + ROPE_DIM)
    wide_q = jnp.concatenate([wide_q[..., :WIDE_NOPE], rotate(wide_q[..., WIDE_NOPE:], positions)], axis=-1)
    narrow_q = narrow_queries.reshape(token_count, NARROW_HEADS, NARROW_NOPE + ROPE_DIM)
    narrow_q = jnp.concatenate([narrow_q[..., :NARROW_NOPE], rotate(narrow_q[..., NARROW_NOPE:], positions)], axis=-1)
    key_rot = rotate(rope_key, positions)
    latent = rms_scale(kv_latent, latent_gain)
    wide_kv = stored(jnp.dot(latent, wide_kv_weight, preferred_element_type=jnp.float32))
    wide_kv = wide_kv.reshape(token_count, WIDE_HEADS, WIDE_NOPE + WIDE_VALUE)
    narrow_kv = stored(jnp.dot(latent, narrow_kv_weight, preferred_element_type=jnp.float32))
    narrow_kv = narrow_kv.reshape(token_count, NARROW_HEADS, NARROW_NOPE + NARROW_VALUE)
    wide_att = attend(wide_q, WIDE_NOPE, wide_kv[..., :WIDE_NOPE], key_rot, wide_kv[..., WIDE_NOPE:])
    narrow_att = attend(narrow_q, NARROW_NOPE, narrow_kv[..., :NARROW_NOPE], key_rot, narrow_kv[..., NARROW_NOPE:])
    wide_per = WIDE_HEADS // N_TP
    narrow_per = NARROW_HEADS // N_TP
    wide_proj = wide_out_weight.reshape(WIDE_HEADS, WIDE_VALUE, D_MODEL).astype(jnp.float32)
    narrow_proj = narrow_out_weight.reshape(NARROW_HEADS, NARROW_VALUE, D_MODEL).astype(jnp.float32)
    proj_total = jnp.zeros((token_count, D_MODEL), jnp.float32)
    for group_index in range(N_TP):
        wide_slice = slice(group_index * wide_per, (group_index + 1) * wide_per)
        narrow_slice = slice(group_index * narrow_per, (group_index + 1) * narrow_per)
        partial_sum = jnp.einsum('thv,hvd->td', wide_att[:, wide_slice].astype(jnp.float32), wide_proj[wide_slice])
        partial_sum = partial_sum + jnp.einsum('thv,hvd->td', narrow_att[:, narrow_slice].astype(jnp.float32), narrow_proj[narrow_slice])
        proj_total = proj_total + stored(partial_sum).astype(jnp.float32)
    attn_proj = stored(proj_total)
    stream = stored(residual.astype(jnp.float32) + attn_proj.astype(jnp.float32))
    normed = rms_scale(stream, norm_gain)
    unit_per = EXPERT_FF // N_TP
    shared_hidden = stored(jax.nn.silu(jnp.dot(normed, shared_gate, preferred_element_type=jnp.float32)) * jnp.dot(normed, shared_up, preferred_element_type=jnp.float32))
    shared_total = jnp.zeros((token_count, D_MODEL), jnp.float32)
    for group_index in range(N_TP):
        unit_slice = slice(group_index * unit_per, (group_index + 1) * unit_per)
        shared_total = shared_total + stored(jnp.dot(shared_hidden[:, unit_slice], shared_down[unit_slice], preferred_element_type=jnp.float32)).astype(jnp.float32)
    shared_out = stored(shared_total)
    flat_ids = route_ids.reshape(-1)
    flat_weights = route_weights.reshape(-1)
    copy_count = token_count * TOP_K
    slot_count = N_SP * CAPACITY

    def visit_expert(routed_acc, expert):
        picked = jnp.nonzero(flat_ids == expert, size=slot_count, fill_value=copy_count)[0].astype(jnp.int32)
        is_live = picked < copy_count
        safe_pick = jnp.minimum(picked, copy_count - 1).astype(jnp.int32)
        token_index = (safe_pick // TOP_K).astype(jnp.int32)
        picked_rows = normed[token_index]
        hidden_units = stored(jax.nn.silu(jnp.dot(picked_rows, expert_gate[expert], preferred_element_type=jnp.float32)) * jnp.dot(picked_rows, expert_up[expert], preferred_element_type=jnp.float32))
        down_weight = expert_down[expert]
        expert_total = jnp.zeros((slot_count, D_MODEL), jnp.float32)
        for group_index in range(N_TP):
            unit_slice = slice(group_index * unit_per, (group_index + 1) * unit_per)
            expert_total = expert_total + stored(jnp.dot(hidden_units[:, unit_slice], down_weight[unit_slice], preferred_element_type=jnp.float32)).astype(jnp.float32)
        expert_result = stored(expert_total).astype(jnp.float32)
        weighting = jnp.where(is_live, flat_weights[safe_pick], 0.0)
        routed_acc = routed_acc.at[token_index].add(weighting[:, None] * expert_result)
        return (routed_acc, None)
    routed, _ = lax.scan(visit_expert, jnp.zeros((token_count, D_MODEL), jnp.float32), jnp.arange(EXPERTS, dtype=jnp.int32))
    return (stream.astype(jnp.float32) + shared_out.astype(jnp.float32) + routed).astype(jnp.bfloat16)
```

```python
import functools

import jax
import jax.numpy as jnp
import numpy as np
from jax import lax
from jax.experimental import pallas as pl
from jax.experimental.pallas import tpu as pltpu
from jax.sharding import Mesh
from jax.sharding import PartitionSpec as P

MESH = pl.DeviceIdType.MESH
ROPE = 32
CAP = 3
SLOTS = 8
THETA = 10000.0
EPS = 1e-06
FLOOR = -1e30
BF = jnp.bfloat16
F32 = jnp.float32


def rotary_table(tokens):
    half = ROPE // 2
    freq = np.float32(THETA) ** (-2.0 * np.arange(half, dtype=np.float32) / np.float32(ROPE))
    freq = freq.astype(np.float32)
    angles = np.arange(tokens, dtype=np.float32)[:, None] * freq[None, :]
    cosine = np.cos(angles.astype(np.float64)).astype(np.float32)
    sine = np.sin(angles.astype(np.float64)).astype(np.float32)
    return np.concatenate([cosine, cosine, -sine, sine], axis=1)


def dot(a, b, ca=1, cb=0):
    return lax.dot_general(a, b, (((ca,), (cb,)), ((), ())), preferred_element_type=F32)


def turned(values, table):
    half = ROPE // 2
    v = values.astype(F32)
    swapped = jnp.concatenate([v[:, half:], v[:, :half]], axis=1)
    return v * table[:, :ROPE] + swapped * table[:, ROPE : 2 * ROPE]


def normalized(values, gain):
    v = values.astype(F32)
    scaled = v * lax.rsqrt(jnp.mean(v * v, axis=-1, keepdims=True) + EPS)
    return (scaled * gain).astype(BF)


def eye(n):
    return lax.broadcasted_iota(jnp.int32, (n, n), 0) == lax.broadcasted_iota(jnp.int32, (n, n), 1)


def upright(line):
    return jnp.sum(jnp.where(eye(line.shape[1]), line, 0.0), axis=1, keepdims=True)


def silu(v):
    return v / (1.0 + jnp.exp(-v))


def shift_of(n):
    return n.bit_length() - 1


def kernel(dims, *refs):
    NZ, NY, NX, TOK, LAT, D, WN, NN = dims
    NT, NS = NY * NX, NZ * 2
    LT, LC, DC = TOK // NY, LAT // NX, D // NT
    KB = NZ * LT
    Q = NS * SLOTS
    RPE = CAP * NS
    ROWS = 2 * RPE
    hbm, out_ref, scratch = refs[:20], refs[20], refs[21:]
    (
        v_wq, v_nq, v_lat, v_rk, v_lg, v_wkv, v_nkv, v_wo, v_no, v_res, v_ng, v_ids, v_rw,
        v_egu, v_ed, v_sgu, v_sd, v_tab,
        latn, rott, zbuf, lat_buf, rot_buf, qlat, qrp, sc,
        pp, rsb, strm, sall, spp, shb, selt, disp, arr, xsend, xall, part, rs2, ret, back,
        lsem, ss, rs, lat_sem,
    ) = scratch
    FF = v_sd.shape[0]
    vmem = [
        v_wq, v_nq, v_lat, v_rk, v_lg, v_wkv, v_nkv, v_wo, v_no, v_res, v_ng, v_ids, v_rw,
        v_egu.at[:, pl.ds(0, FF)], v_egu.at[:, pl.ds(FF, FF)], v_ed,
        v_sgu.at[pl.ds(0, FF)], v_sgu.at[pl.ds(FF, FF)], v_sd, v_tab,
    ]

    z, c = lax.axis_index("z"), lax.axis_index("c")
    y, x = lax.axis_index("y"), lax.axis_index("x")
    t = y * NX + x
    s = z * 2 + c

    def plane(k):
        t2 = (t + k) % NT
        return {"y": t2 // NX, "x": t2 % NX}, t2

    def seq(k):
        s2 = (s + k) % NS
        return {"z": s2 // 2, "c": s2 % 2}, s2

    def cols(i):
        return pl.ds(pl.multiple_of(i * DC, DC), DC)

    def send(src, dst, ssem, rsem, dev):
        pltpu.make_async_remote_copy(
            src_ref=src, dst_ref=dst, send_sem=ssem, recv_sem=rsem, device_id=dev, device_id_type=MESH
        ).start()

    def wait(ref, sem):
        pltpu.make_async_copy(ref, ref, sem).wait()

    def each(lo, hi, f):
        def body(k, carry):
            f(k)
            return carry

        lax.fori_loop(lo, hi, body, 0)

    bar = pltpu.get_barrier_semaphore()
    each(1, NS, lambda k: pl.semaphore_signal(bar, inc=1, device_id=seq(k)[0], device_id_type=MESH))
    each(1, NT, lambda k: pl.semaphore_signal(bar, inc=1, device_id=plane(k)[0], device_id_type=MESH))

    loads = []
    for i in range(20):
        src = hbm[i]
        if i == 9:
            src = src.at[:, cols(t)]
        if i == 19:
            src = src.at[pl.ds(pl.multiple_of(s * TOK, TOK), TOK)]
        loads.append(pltpu.make_async_copy(src, vmem[i], lsem.at[i]))
    for i in (2, 3, 4, 19, 0, 1, 5, 6, 11, 12, 9, 7, 8, 10, 16, 17, 18, 13, 14, 15):
        loads[i].start()

    for i in (2, 3, 4, 19):
        loads[i].wait()
    table = v_tab[...]
    latn[...] = normalized(v_lat[...], v_lg[...])
    rk = turned(dot(v_rk[...], eye(ROPE).astype(BF), 0, 0), table)
    rott[...] = jnp.concatenate([rk[i * LT : (i + 1) * LT] for i in range(NY)], axis=1).astype(BF)

    pl.semaphore_wait(bar, NS + NT - 2)

    own_tile = latn.at[pl.ds(pl.multiple_of(y * LT, LT), LT), pl.ds(pl.multiple_of(x * LC, LC), LC)]
    zslot = zbuf.at[pl.ds(pl.multiple_of(z * LT, LT), LT)]
    rslot = zbuf.at[pl.ds(KB, LT)]

    def z_send(k):
        z2 = (z + k) % NZ
        send(own_tile, zslot, ss.at[0], rs.at[0], {"z": z2})

    def r_send(k):
        z2 = (z + k) % NZ
        send(rott, rslot, ss.at[1], rs.at[1], {"z": z2})

    each(1, NZ, z_send)
    pltpu.make_async_copy(own_tile, zslot, rs.at[0]).start()

    @pl.when(z == t)
    def _():
        each(1, NZ, r_send)
        pltpu.make_async_copy(rott, rslot, rs.at[1]).start()

    for i in (0, 1, 5, 6):
        loads[i].wait()
    wscale, nscale = (WN + ROPE) ** -0.5, (NN + ROPE) ** -0.5
    qlat[:TOK] = (dot(v_wq[:, :WN], v_wkv[:, :WN], 1, 1) * wscale).astype(BF)
    qlat[TOK:] = (dot(v_nq[:, :NN], v_nkv[:, :NN], 1, 1) * nscale).astype(BF)
    qr = jnp.concatenate(
        [turned(v_wq[:, WN:], table) * wscale, turned(v_nq[:, NN:], table) * nscale], axis=0
    )
    for i in range(NY):
        parts = []
        if i:
            parts.append(jnp.zeros((2 * TOK, ROPE * i), F32))
        parts.append(qr)
        if i < NY - 1:
            parts.append(jnp.zeros((2 * TOK, ROPE * (NY - 1 - i)), F32))
        qrp[i] = jnp.concatenate(parts, axis=1).astype(BF)

    for i in (11, 12):
        loads[i].wait()
    lane = lax.broadcasted_iota(jnp.int32, (TOK, Q), 1)
    j = lane & (SLOTS - 1)
    high = (j >= CAP).astype(jnp.int32)
    expert = (lane >> shift_of(SLOTS)) * 2 + high
    hit0 = upright(v_ids[0:1].astype(F32)) == expert.astype(F32)
    hit1 = upright(v_ids[1:2].astype(F32)) == expert.astype(F32)
    ahead = (
        lax.broadcasted_iota(jnp.int32, (TOK, TOK), 0) > lax.broadcasted_iota(jnp.int32, (TOK, TOK), 1)
    ).astype(F32)
    hits = jnp.where(hit0 | hit1, 1.0, 0.0).astype(F32)
    rank = dot(ahead.astype(BF), hits.astype(BF))
    fits = (rank == (j - CAP * high).astype(F32)) & (j < 2 * CAP)
    selt[0] = jnp.where(hit0 & fits, 1.0, 0.0).astype(BF)
    selt[1] = jnp.where(hit1 & fits, 1.0, 0.0).astype(BF)

    wait(zbuf.at[pl.ds(0, KB)], rs.at[0])
    wait(rslot, rs.at[1])
    zlat = zbuf.at[pl.ds(0, KB)]

    def lat_slot(p, t2):
        return lat_buf.at[p, t2 // NX, :, pl.ds(pl.multiple_of((t2 % NX) * LC, LC), LC)]

    my_rot = rot_buf.at[c, pl.ds(pl.multiple_of(t * LT, LT), LT)]
    pltpu.make_async_copy(zlat, lat_slot(c, t), lat_sem.at[0]).start()
    pltpu.make_async_copy(rslot, my_rot, rs.at[2]).start()

    def p_send(k):
        dev, _ = plane(k)
        send(zlat, lat_slot(c, t), ss.at[2], lat_sem.at[k], dev)
        send(rslot, my_rot, ss.at[3], rs.at[2], dev)

    each(1, NT, p_send)
    other = {"c": 1 - c}

    def relay(k):
        t2 = (t + NT - k) % NT
        wait(zlat, lat_sem.at[k])
        send(lat_slot(c, t2), lat_slot(c, t2), ss.at[4], rs.at[3], other)

    each(0, NT, relay)
    wait(rot_buf.at[c], rs.at[2])
    send(rot_buf.at[c], rot_buf.at[c], ss.at[5], rs.at[4], other)
    wait(lat_buf.at[1 - c], rs.at[3])
    wait(rot_buf.at[1 - c], rs.at[4])

    key = lax.broadcasted_iota(jnp.int32, (2 * TOK, KB), 1)
    key_at = (key >> shift_of(LT)) * (2 * TOK) + (key & (LT - 1))
    query_at = s * TOK + (lax.broadcasted_iota(jnp.int32, (2 * TOK, KB), 0) & (TOK - 1))
    ahead_by = query_at - key_at
    peak = jnp.full((2 * TOK, 1), FLOOR, F32)
    ql = qlat[...]
    for p in range(2):
        for i in range(NY):
            scores = dot(ql, lat_buf[p, i], 1, 1) + dot(qrp[i], rot_buf[p], 1, 1)
            scores = jnp.where(ahead_by >= p * TOK + i * LT, scores, FLOOR)
            sc[p * NY + i] = scores
            peak = jnp.maximum(peak, jnp.max(scores, axis=-1, keepdims=True))
    total = jnp.zeros((2 * TOK, 1), F32)
    mixed = jnp.zeros((2 * TOK, LAT), F32)
    for p in range(2):
        for i in range(NY):
            probs = jnp.exp(sc[p * NY + i] - peak)
            total = total + jnp.sum(probs, axis=-1, keepdims=True)
            mixed = mixed + dot(probs.astype(BF), lat_buf[p, i])
    mixed = (mixed / total).astype(BF)
    wide = dot(mixed[:TOK], v_wkv[:, WN:]).astype(BF)
    narrow = dot(mixed[TOK:], v_nkv[...])[:, NN:].astype(BF)
    for i in (7, 8, 9):
        loads[i].wait()
    pp[...] = (dot(wide, v_wo[...]) + dot(narrow, v_no[...])).astype(BF)

    def pp_send(k):
        dev, t2 = plane(k)
        send(pp.at[:, cols(t2)], rsb.at[k - 1], ss.at[6], rs.at[5], dev)

    each(1, NT, pp_send)
    acc = pp[:, cols(t)].astype(F32)
    wait(rsb, rs.at[5])
    for k in range(NT - 1):
        acc = acc + rsb[k].astype(F32)
    stream = (v_res[...].astype(F32) + acc.astype(BF).astype(F32)).astype(BF)
    strm[...] = stream

    sel_all = selt[0] + selt[1]
    disp[...] = dot(sel_all, stream, 0, 0).reshape(NS, SLOTS, DC).astype(BF)

    def d_send(k):
        dev, s2 = seq(k)
        send(disp.at[s2], arr.at[s], ss.at[7], rs.at[6], dev)

    each(1, NS, d_send)
    pltpu.make_async_copy(disp.at[s], arr.at[s], rs.at[6]).start()

    def s_send(k):
        dev, _ = plane(k)
        send(strm, sall.at[:, cols(t)], ss.at[8], rs.at[7], dev)

    each(1, NT, s_send)
    pltpu.make_async_copy(strm, sall.at[:, cols(t)], rs.at[7]).start()

    for i in (10, 16, 17, 18):
        loads[i].wait()
    wait(sall, rs.at[7])
    gain = v_ng[...]
    normed = normalized(sall[...], gain)
    both = dot(normed, v_sgu[...], 1, 1)
    hidden = (silu(both[:, :FF]) * both[:, FF:]).astype(BF)
    spp[...] = dot(hidden, v_sd[...]).astype(BF)

    def sh_send(k):
        dev, t2 = plane(k)
        send(spp.at[:, cols(t2)], shb.at[k - 1], ss.at[9], rs.at[8], dev)

    each(1, NT, sh_send)

    wait(arr, rs.at[6])
    row = lax.broadcasted_iota(jnp.int32, (ROWS, Q), 0)
    slot = lax.broadcasted_iota(jnp.int32, (ROWS, Q), 1)
    pick = jnp.where(slot == (row & (NS - 1)) * SLOTS + (row >> shift_of(NS)), 1.0, 0.0).astype(BF)
    xsend[...] = dot(pick, arr[...].astype(F32).reshape(Q, DC).astype(BF)).astype(BF)

    def x_send(k):
        dev, _ = plane(k)
        send(xsend, xall.at[:, cols(t)], ss.at[10], rs.at[9], dev)

    each(1, NT, x_send)
    pltpu.make_async_copy(xsend, xall.at[:, cols(t)], rs.at[9]).start()
    for i in (13, 14, 15):
        loads[i].wait()
    wait(xall, rs.at[9])
    for e in range(2):
        rows = normalized(xall[e * RPE : (e + 1) * RPE], gain)
        both = dot(rows, v_egu[e], 1, 1)
        hidden = (silu(both[:, :FF]) * both[:, FF:]).astype(BF)
        part[e * RPE : (e + 1) * RPE] = dot(hidden, v_ed[e]).astype(BF)

    def e_send(k):
        dev, t2 = plane(k)
        send(part.at[:, cols(t2)], rs2.at[k - 1], ss.at[11], rs.at[10], dev)

    each(1, NT, e_send)
    acc = part[:, cols(t)].astype(F32)

    shared = spp[:, cols(t)].astype(F32)
    wait(shb, rs.at[8])
    for k in range(NT - 1):
        shared = shared + shb[k].astype(F32)
    shared = shared.astype(BF).astype(F32)

    wait(rs2, rs.at[10])
    for k in range(NT - 1):
        acc = acc + rs2[k].astype(F32)
    row = lax.broadcasted_iota(jnp.int32, (Q, ROWS), 1)
    slot = lax.broadcasted_iota(jnp.int32, (Q, ROWS), 0)
    unpick = jnp.where(slot == (row & (NS - 1)) * SLOTS + (row >> shift_of(NS)), 1.0, 0.0).astype(BF)
    ret[...] = dot(unpick, acc.astype(BF)).reshape(NS, SLOTS, DC).astype(BF)

    def b_send(k):
        dev, s2 = seq(k)
        send(ret.at[s2], back.at[s], ss.at[12], rs.at[11], dev)

    each(1, NS, b_send)
    pltpu.make_async_copy(ret.at[s], back.at[s], rs.at[11]).start()
    wait(back, rs.at[11])
    rows = back[...].astype(F32).reshape(Q, DC).astype(BF)
    routed = dot(selt[0], rows) * upright(v_rw[0:1]) + dot(selt[1], rows) * upright(v_rw[1:2])
    out_ref[...] = (strm[...].astype(F32) + shared + routed).astype(BF)

    wait(zbuf.at[pl.ds(0, (NZ - 1) * LT)], ss.at[0])

    @pl.when(z == t)
    def _():
        wait(zbuf.at[pl.ds(0, (NZ - 1) * LT)], ss.at[1])

    each(1, NT, lambda k: wait(zlat, ss.at[2]))
    wait(rot_buf.at[0, pl.ds(0, (NT - 1) * LT)], ss.at[3])
    wait(lat_buf.at[0], ss.at[4])
    wait(rot_buf.at[0], ss.at[5])
    wait(rsb, ss.at[6])
    wait(disp.at[pl.ds(0, NS - 1)], ss.at[7])
    wait(rsb, ss.at[8])
    wait(shb, ss.at[9])
    wait(rs2, ss.at[10])
    wait(rs2, ss.at[11])
    wait(ret.at[pl.ds(0, NS - 1)], ss.at[12])


def local(dims, interpret, *args):
    NZ, NY, NX, TOK, LAT, D, WN, NN = dims
    NT, NS = NY * NX, NZ * 2
    LT, LC, DC = TOK // NY, LAT // NX, D // NT
    KB = NZ * LT
    Q = NS * SLOTS
    ROWS = 2 * CAP * NS
    args = list(args)
    args[4] = args[4].reshape(1, -1)
    args[10] = args[10].reshape(1, -1)
    for i in (3, 11, 12, 13, 14, 16, 17):
        args[i] = jnp.swapaxes(args[i], -1, -2)
    FF = args[18].shape[0]
    args.append(jnp.asarray(rotary_table(NS * TOK)))
    shapes = [a.shape for a in args]
    shapes[9] = (TOK, DC)
    shapes[19] = (TOK, 2 * ROPE)
    shapes[13] = (2, 2 * FF, D)
    shapes[16] = (2 * FF, D)
    kept = [i for i in range(20) if i not in (14, 17)]
    scratch = [pltpu.VMEM(shapes[i], args[i].dtype) for i in kept]
    scratch += [
        pltpu.VMEM((TOK, LAT), BF),
        pltpu.VMEM((LT, ROPE * NY), BF),
        pltpu.VMEM((KB + LT, LC), BF),
        pltpu.VMEM((2, NY, KB, LAT), BF),
        pltpu.VMEM((2, KB, ROPE * NY), BF),
        pltpu.VMEM((2 * TOK, LAT), BF),
        pltpu.VMEM((NY, 2 * TOK, ROPE * NY), BF),
        pltpu.VMEM((2 * NY, 2 * TOK, KB), F32),
        pltpu.VMEM((TOK, D), BF),
        pltpu.VMEM((NT - 1, TOK, DC), BF),
        pltpu.VMEM((TOK, DC), BF),
        pltpu.VMEM((TOK, D), BF),
        pltpu.VMEM((TOK, D), BF),
        pltpu.VMEM((NT - 1, TOK, DC), BF),
        pltpu.VMEM((2, TOK, Q), BF),
        pltpu.VMEM((NS, SLOTS, DC), BF),
        pltpu.VMEM((NS, SLOTS, DC), BF),
        pltpu.VMEM((ROWS, DC), BF),
        pltpu.VMEM((ROWS, D), BF),
        pltpu.VMEM((ROWS, D), BF),
        pltpu.VMEM((NT - 1, ROWS, DC), BF),
        pltpu.VMEM((NS, SLOTS, DC), BF),
        pltpu.VMEM((NS, SLOTS, DC), BF),
        pltpu.SemaphoreType.DMA((20,)),
        pltpu.SemaphoreType.DMA((13,)),
        pltpu.SemaphoreType.DMA((12,)),
        pltpu.SemaphoreType.DMA((NT,)),
    ]
    return pl.pallas_call(
        functools.partial(kernel, dims),
        out_shape=jax.ShapeDtypeStruct((TOK, DC), BF),
        in_specs=[pl.BlockSpec(memory_space=pl.ANY)] * 20,
        out_specs=pl.BlockSpec(memory_space=pltpu.VMEM),
        scratch_shapes=scratch,
        compiler_params=pltpu.CompilerParams(
            collective_id=0, has_side_effects=True, vmem_limit_bytes=60 * 1024 * 1024
        ),
        name="layer",
    )(*args)


def build(mesh, nz, ny, nx, tok, lat, d, wn, nn):
    torus = Mesh(mesh.devices.reshape(nz, 2, ny, nx), ("z", "c", "y", "x"))
    SP, TP = ("z", "c"), ("y", "x")
    return jax.shard_map(
        functools.partial(local, (nz, ny, nx, tok, lat, d, wn, nn), False),
        mesh=torus,
        in_specs=(
            P(SP, TP),
            P(SP, TP),
            P(SP, None),
            P(SP, None),
            P(),
            P(None, TP),
            P(None, TP),
            P(TP, None),
            P(TP, None),
            P(SP, None),
            P(),
            P(SP, None),
            P(SP, None),
            P(SP, None, TP),
            P(SP, None, TP),
            P(SP, TP, None),
            P(None, TP),
            P(None, TP),
            P(TP, None),
        ),
        out_specs=P(SP, TP),
        check_vma=False,
    )


def solution(mesh):
    return build(mesh, 16, 4, 4, 64, 512, 2048, 128, 64)
```

```python
import functools

import jax
import jax.numpy as jnp
import numpy as np
from jax import lax
from jax.experimental import pallas as pl
from jax.experimental.pallas import tpu as pltpu
from jax.sharding import Mesh
from jax.sharding import PartitionSpec as P

MESH = pl.DeviceIdType.MESH
ROPE = 32
CAP = 3
SLOTS = 8
THETA = 10000.0
EPS = 1e-06
FLOOR = -1e30
BF = jnp.bfloat16
F32 = jnp.float32


def rotary_table(tokens):
    half = ROPE // 2
    freq = np.float32(THETA) ** (-2.0 * np.arange(half, dtype=np.float32) / np.float32(ROPE))
    freq = freq.astype(np.float32)
    angles = np.arange(tokens, dtype=np.float32)[:, None] * freq[None, :]
    cosine = np.cos(angles.astype(np.float64)).astype(np.float32)
    sine = np.sin(angles.astype(np.float64)).astype(np.float32)
    return np.concatenate([cosine, cosine, -sine, sine], axis=1)


def dot(a, b, ca=1, cb=0):
    return lax.dot_general(a, b, (((ca,), (cb,)), ((), ())), preferred_element_type=F32)


def turned(values, table):
    half = ROPE // 2
    v = values.astype(F32)
    swapped = jnp.concatenate([v[:, half:], v[:, :half]], axis=1)
    return v * table[:, :ROPE] + swapped * table[:, ROPE : 2 * ROPE]


def normalized(values, gain):
    v = values.astype(F32)
    scaled = v * lax.rsqrt(jnp.mean(v * v, axis=-1, keepdims=True) + EPS)
    return (scaled * gain).astype(BF)


def eye(n):
    return lax.broadcasted_iota(jnp.int32, (n, n), 0) == lax.broadcasted_iota(jnp.int32, (n, n), 1)


def upright(line):
    return jnp.sum(jnp.where(eye(line.shape[1]), line, 0.0), axis=1, keepdims=True)


def silu(v):
    return v / (1.0 + jnp.exp(-v))


def shift_of(n):
    return n.bit_length() - 1


def kernel(dims, *refs):
    NZ, NY, NX, TOK, LAT, D, WN, NN, NG = dims
    NT, NS = NY * NX, NZ * 2
    LT, LC, DC = TOK // NY, LAT // NX, D // NT
    GZ = NZ // NG
    CH = GZ * LT
    KB = NY * CH
    HS = NS // NG
    Q = NS * SLOTS
    HQ = HS * SLOTS
    RPE = CAP * HS
    ROWS = 2 * RPE
    hbm, out_ref, scratch = refs[:20], refs[20], refs[21:]
    (
        v_wq, v_nq, v_lat, v_rk, v_lg, v_wkv, v_nkv, v_wo, v_no, v_res, v_ng, v_ids, v_rw,
        v_egu, v_ed, v_sgu, v_sd, v_tab,
        latn, rott, zbuf, zrot, lat_buf, rot_buf, qlat, qrp, mixd,
        pp, rsb, strm, sall, spp, shb, selt, disp, arr, xsend, xall, part, rs2, ret, back,
        lsem, ss, rs, zsem, zsend, rsend, psem, psend, qsem, csem, csend, dsem, dsend, asem, xsem, esem,
    ) = scratch
    FF = v_sd.shape[0]
    vmem = [
        v_wq, v_nq, v_lat, v_rk, v_lg, v_wkv, v_nkv, v_wo, v_no, v_res, v_ng, v_ids, v_rw,
        v_egu.at[0], v_egu.at[1], v_ed,
        v_sgu.at[pl.ds(0, FF)], v_sgu.at[pl.ds(FF, FF)], v_sd, v_tab,
    ]

    z, c = lax.axis_index("z"), lax.axis_index("c")
    y, x = lax.axis_index("y"), lax.axis_index("x")
    t = y * NX + x
    s = z * 2 + c
    gz = lax.div(z, GZ)

    def plane(k):
        t2 = lax.rem(t + k, NT)
        return {"y": lax.div(t2, NX), "x": lax.rem(t2, NX)}, t2

    def seq(k):
        s2 = lax.rem(s + k + NS // 4, NS)
        return {"z": lax.div(s2, 2), "c": lax.rem(s2, 2)}, s2

    def others(f):
        each(0, NS - NS // 4, f)
        each(NS - NS // 4 + 1, NS, f)

    def cols(i):
        return pl.ds(pl.multiple_of(i * DC, DC), DC)

    def send(src, dst, ssem, rsem, dev):
        pltpu.make_async_remote_copy(
            src_ref=src, dst_ref=dst, send_sem=ssem, recv_sem=rsem, device_id=dev, device_id_type=MESH
        ).start()

    def keep(src, dst, sem):
        pltpu.make_async_copy(src, dst, sem).start()

    def wait(ref, sem, name="w"):
        with jax.named_scope(name):
            pltpu.make_async_copy(ref, ref, sem).wait()

    def each(lo, hi, f):
        def body(k, carry):
            f(k)
            return carry

        lax.fori_loop(lo, hi, body, 0)

    bar = pltpu.get_barrier_semaphore()
    others(lambda k: pl.semaphore_signal(bar, inc=1, device_id=seq(k)[0], device_id_type=MESH))
    each(1, NT, lambda k: pl.semaphore_signal(bar, inc=1, device_id=plane(k)[0], device_id_type=MESH))

    loads = []
    for i in range(20):
        src = hbm[i]
        if i == 9:
            src = src.at[:, cols(t)]
        if i == 19:
            src = src.at[pl.ds(pl.multiple_of(s * TOK, TOK), TOK)]
        loads.append(pltpu.make_async_copy(src, vmem[i], lsem.at[i]))
    for i in (2, 3, 4, 19, 0, 1, 5, 6, 11, 12, 9, 7, 8, 10, 16, 17, 18, 13, 14, 15):
        loads[i].start()

    def loaded(*which):
        for i in which:
            loads[i].wait()

    def clear_tile(i):
        zbuf[gz, pl.ds(pl.multiple_of(i * LT, LT), LT)] = jnp.zeros((LT, LC), BF)

    def clear_turn(i):
        rot_buf[c, pl.ds(pl.multiple_of(i * LT, LT), LT)] = jnp.zeros((LT, ROPE * NY), BF)

    each(lax.rem(z, GZ) + 1, GZ, clear_tile)
    each(z + 1, NZ, clear_turn)

    loaded(2, 3, 4, 19)
    table = v_tab[...]
    latn[...] = normalized(v_lat[...], v_lg[...])
    rk = turned(dot(v_rk[...], eye(ROPE).astype(BF), 0, 0), table)
    rott[...] = jnp.concatenate([rk[i * LT : (i + 1) * LT] for i in range(NY)], axis=1).astype(BF)

    with jax.named_scope("w_bar"):
        pl.semaphore_wait(bar, NS + NT - 2)

    own_tile = latn.at[pl.ds(pl.multiple_of(y * LT, LT), LT), pl.ds(pl.multiple_of(x * LC, LC), LC)]
    zslot = zbuf.at[gz, pl.ds(pl.multiple_of(lax.rem(z, GZ) * LT, LT), LT)]

    each(1, NZ - z, lambda k: send(own_tile, zslot, zsend.at[k], zsem.at[z], {"z": z + k}))
    keep(own_tile, zslot, zsem.at[z])

    @pl.when(z == t)
    def _():
        each(1, NZ - z, lambda k: send(rott, zrot, rsend.at[k], rs.at[1], {"z": z + k}))
        keep(rott, zrot, rs.at[1])

    loaded(0, 1, 5, 6)
    wscale, nscale = (WN + ROPE) ** -0.5, (NN + ROPE) ** -0.5
    qlat[:TOK] = (dot(v_wq[:, :WN], v_wkv[:, :WN], 1, 1) * wscale).astype(BF)
    qlat[TOK:] = (dot(v_nq[:, :NN], v_nkv[:, :NN], 1, 1) * nscale).astype(BF)
    qr = jnp.concatenate(
        [turned(v_wq[:, WN:], table) * wscale, turned(v_nq[:, NN:], table) * nscale], axis=0
    )
    qrp[...] = jnp.concatenate([qr] * NY, axis=1).astype(BF)

    def lat_slot(g):
        return lat_buf.at[
            c, g, pl.ds(pl.multiple_of(y * CH, CH), CH), pl.ds(pl.multiple_of(x * LC, LC), LC)
        ]

    top = lax.div(gz, NG - 1)

    def group(k):
        first = lax.div(NG - k, NG)
        second = lax.div(NG + 1 - k, NG) - first
        return top * (first * gz + (1 - first - second) * (NG - k)) + (1 - top) * (gz - k)

    my_rot = rot_buf.at[c, pl.ds(pl.multiple_of(t * LT, LT), LT)]

    def tiles_of(g, k):
        lo = g * GZ
        whole = 1 - lax.div(NG - k, NG)
        return lo, lo + whole * GZ + (1 - whole) * (lax.rem(z, GZ) + 1)

    def group_out(k):
        g = group(k)
        each(*tiles_of(g, k), lambda i: wait(zslot, zsem.at[i], "w_z"))

        @pl.when((lax.div(t, GZ) == g) & (t <= z))
        def _():
            wait(zrot, rs.at[1], "w_zrot")
            keep(zrot, my_rot, qsem.at[t])
            each(1, NT, lambda i: send(zrot, my_rot, ss.at[3], qsem.at[t], plane(i)[0]))

        keep(zbuf.at[g], lat_slot(g), psem.at[g])
        each(1, NT, lambda i: send(zbuf.at[g], lat_slot(g), psend.at[g], psem.at[g], plane(i)[0]))

    each(0, gz + 1, group_out)

    loaded(11, 12)
    lane = lax.broadcasted_iota(jnp.int32, (TOK, Q), 1)
    j = lane & (SLOTS - 1)
    high = (j >= CAP).astype(jnp.int32)
    expert = ((lane >> shift_of(SLOTS)) * 2 + high).astype(F32)
    hit0 = upright(v_ids[0:1].astype(F32)) == expert
    hit1 = upright(v_ids[1:2].astype(F32)) == expert
    ahead = (
        lax.broadcasted_iota(jnp.int32, (TOK, TOK), 0) > lax.broadcasted_iota(jnp.int32, (TOK, TOK), 1)
    ).astype(F32)
    hits = jnp.where(hit0 | hit1, 1.0, 0.0).astype(F32)
    rank = dot(ahead.astype(BF), hits.astype(BF))
    fits = (rank == (j - CAP * high).astype(F32)) & (j < 2 * CAP)
    selt[0] = jnp.where(hit0 & fits, 1.0, 0.0).astype(BF)
    selt[1] = jnp.where(hit1 & fits, 1.0, 0.0).astype(BF)

    other = {"c": 1 - c}

    def turn_rows(p, g):
        return rot_buf.at[p, pl.ds(pl.multiple_of(g * CH, CH), CH)]

    def group_over(k):
        g = group(k)
        wait(lat_buf.at[c, g], psem.at[g], "w_plane")
        send(lat_buf.at[c, g], lat_buf.at[c, g], csend.at[g], csem.at[g], other)
        each(*tiles_of(g, k), lambda i: wait(zrot, qsem.at[i], "w_prot"))
        send(turn_rows(c, g), turn_rows(c, g), dsend.at[g], dsem.at[g], other)

    key = lax.broadcasted_iota(jnp.int32, (2 * TOK, KB), 1)
    key_at = (
        (key >> shift_of(CH)) * LT + ((key >> shift_of(LT)) & (GZ - 1)) * (2 * TOK) + (key & (LT - 1))
    )
    query_at = s * TOK + (lax.broadcasted_iota(jnp.int32, (2 * TOK, KB), 0) & (TOK - 1))
    ahead_by = query_at - key_at
    strip = lax.broadcasted_iota(jnp.int32, (CH, ROPE * NY), 1) >> shift_of(ROPE)
    mixd[...] = jnp.zeros_like(mixd)

    def attend(p, g, carry):
        peak, total = carry
        turns = rot_buf[p, pl.ds(pl.multiple_of(g * CH, CH), CH)].astype(F32)
        turns = jnp.concatenate([jnp.where(strip == i, turns, 0.0) for i in range(NY)], axis=0)
        keys = lat_buf[p, g]
        scores = dot(qlat[...], keys, 1, 1) + dot(qrp[...], turns.astype(BF), 1, 1)
        scores = jnp.where(ahead_by >= p * TOK + g * (GZ * 2 * TOK), scores, FLOOR)
        newest = jnp.maximum(peak, jnp.max(scores, axis=-1, keepdims=True))
        fade = jnp.exp(peak - newest)
        probs = jnp.exp(scores - newest)
        mixd[...] = mixd[...] * fade + dot(probs.astype(BF), keys)
        return newest, total * fade + jnp.sum(probs, axis=-1, keepdims=True)

    def other_attend(k, carry):
        g = group(k)
        wait(lat_buf.at[1 - c, g], csem.at[g], "w_core")
        wait(turn_rows(1 - c, g), dsem.at[g], "w_crot")
        return attend(1 - c, g, carry)

    def both_attend(k, carry):
        group_over(k)
        carry = attend(c, group(k), carry)
        return lax.fori_loop(jnp.maximum(k - 1, 0), k, other_attend, carry)

    carry = (jnp.full((2 * TOK, 1), FLOOR, F32), jnp.zeros((2 * TOK, 1), F32))
    carry = lax.fori_loop(0, gz + 1, both_attend, carry)
    _, total = lax.fori_loop(gz, gz + 1, other_attend, carry)
    mixed = (mixd[...] / total).astype(BF)
    wide = dot(mixed[:TOK], v_wkv[:, WN:]).astype(BF)
    narrow = dot(mixed[TOK:], v_nkv[...])[:, NN:].astype(BF)
    loaded(7, 8, 9)
    pp[...] = (dot(wide, v_wo[...]) + dot(narrow, v_no[...])).astype(BF)

    late = z >= GZ

    def spread(rows, slots, r_axis):
        row = lax.broadcasted_iota(jnp.int32, (rows, slots), r_axis)
        slot = lax.broadcasted_iota(jnp.int32, (rows, slots), 1 - r_axis)
        return jnp.where(slot == (row & (HS - 1)) * SLOTS + (row >> shift_of(HS)), 1.0, 0.0).astype(BF)

    def rows_out(h):
        wait(arr.at[pl.ds(h * HS, HS)], asem.at[h], f"w_arr{h}")
        came = arr[h * HS : (h + 1) * HS].astype(F32).reshape(HQ, DC).astype(BF)
        xsend[h] = dot(spread(ROWS, HQ, 0), came).astype(BF)
        each(1, NT, lambda k: send(xsend.at[h], xall.at[h, :, cols(t)], ss.at[10], xsem.at[h], plane(k)[0]))
        keep(xsend.at[h], xall.at[h, :, cols(t)], xsem.at[h])

    def experts(h):
        wait(xall.at[h], xsem.at[h], f"w_xall{h}")
        both = dot(normalized(xall[h], v_ng[...]), v_egu[...].reshape(4 * FF, D), 1, 1)
        hidden = silu(both[:, : 2 * FF]) * both[:, 2 * FF :]
        first = lax.broadcasted_iota(jnp.int32, (ROWS, 2 * FF), 0) < RPE
        hidden = jnp.where(first == (lax.broadcasted_iota(jnp.int32, (ROWS, 2 * FF), 1) < FF), hidden, 0.0)
        part[h] = dot(hidden.astype(BF), v_ed[...].reshape(2 * FF, D)).astype(BF)

        def e_send(k):
            dev, t2 = plane(k)
            send(part.at[h, :, cols(t2)], rs2.at[h, k - 1], ss.at[11], esem.at[h], dev)

        each(1, NT, e_send)

    def rows_back(h):
        acc = part[h, :, cols(t)].astype(F32)
        wait(rs2.at[h], esem.at[h], f"w_rs2_{h}")
        for k in range(NT - 1):
            acc = acc + rs2[h, k].astype(F32)
        ret[h] = dot(spread(HQ, ROWS, 1), acc.astype(BF)).reshape(HS, SLOTS, DC).astype(BF)

        def b_send(k):
            r2 = lax.rem(s + k, HS)
            s2 = h * HS + r2

            @pl.when(s2 != s)
            def _():
                send(ret.at[h, r2], back.at[s], ss.at[12], rs.at[11], {"z": lax.div(s2, 2), "c": lax.rem(s2, 2)})

            @pl.when(s2 == s)
            def _():
                keep(ret.at[h, r2], back.at[s], rs.at[11])

        each(0, HS, b_send)

    def pp_send(k):
        dev, t2 = plane(k)
        send(pp.at[:, cols(t2)], rsb.at[k - 1], ss.at[6], rs.at[5], dev)

    each(1, NT, pp_send)
    loaded(10, 16, 17, 18, 13, 14, 15)

    @pl.when(late)
    def _():
        rows_out(0)

    acc = pp[:, cols(t)].astype(F32)
    wait(rsb, rs.at[5], "w_proj")
    for k in range(NT - 1):
        acc = acc + rsb[k].astype(F32)
    stream = (v_res[...].astype(F32) + acc.astype(BF).astype(F32)).astype(BF)
    strm[...] = stream

    bunch = lax.div(s, HS)
    disp[...] = dot(selt[0] + selt[1], stream, 0, 0).reshape(NS, SLOTS, DC).astype(BF)

    def d_send(k):
        dev, s2 = seq(k)
        send(disp.at[s2], arr.at[s], ss.at[7], asem.at[bunch], dev)

    others(d_send)
    keep(disp.at[s], arr.at[s], asem.at[bunch])

    def stream_out():
        each(1, NT, lambda k: send(strm, sall.at[:, cols(t)], ss.at[8], rs.at[7], plane(k)[0]))
        keep(strm, sall.at[:, cols(t)], rs.at[7])

    def shared_expert():
        wait(sall, rs.at[7], "w_sall")
        both = dot(normalized(sall[...], v_ng[...]), v_sgu[...], 1, 1)
        hidden = (silu(both[:, :FF]) * both[:, FF:]).astype(BF)
        spp[...] = dot(hidden, v_sd[...]).astype(BF)

    def shared_out():
        def sh_send(k):
            dev, t2 = plane(k)
            send(spp.at[:, cols(t2)], shb.at[k - 1], ss.at[9], rs.at[8], dev)

        each(1, NT, sh_send)

    @pl.when(jnp.logical_not(late))
    def _():
        stream_out()
        shared_expert()
        rows_out(0)
        shared_out()

    rows_out(1)
    experts(0)
    for h in range(2, NG):
        rows_out(h)
    for h in range(1, NG):
        experts(h)
        if h < NG - 1:
            rows_back(h - 1)

    @pl.when(late)
    def _():
        stream_out()

    for h in range(NG - 2, NG):
        rows_back(h)

    @pl.when(late)
    def _():
        shared_expert()
        shared_out()

    shared = spp[:, cols(t)].astype(F32)
    wait(shb, rs.at[8], "w_shb")
    for k in range(NT - 1):
        shared = shared + shb[k].astype(F32)
    before = strm[...].astype(F32) + shared.astype(BF).astype(F32)

    wait(back, rs.at[11], "w_back")
    rows = back[...].astype(F32).reshape(Q, DC).astype(BF)
    routed = dot(selt[0], rows) * upright(v_rw[0:1]) + dot(selt[1], rows) * upright(v_rw[1:2])
    out_ref[...] = (before + routed).astype(BF)

    each(1, NZ - z, lambda k: wait(zslot, zsend.at[k]))

    @pl.when(z == t)
    def _():
        each(1, NZ - z, lambda k: wait(zrot, rsend.at[k]))

    each(0, gz + 1, lambda g: wait(lat_buf.at[0, 0, pl.ds(0, KB * (NT - 1) // NT)], psend.at[g]))

    @pl.when(t <= z)
    def _():
        wait(rot_buf.at[0, pl.ds(0, (NT - 1) * LT)], ss.at[3])

    each(0, gz + 1, lambda g: wait(lat_buf.at[0, 0], csend.at[g]))
    each(0, gz + 1, lambda g: wait(turn_rows(0, 0), dsend.at[g]))
    wait(rsb, ss.at[6])
    wait(disp.at[pl.ds(0, NS - 1)], ss.at[7])
    wait(rsb, ss.at[8])
    wait(shb, ss.at[9])
    wait(rs2, ss.at[10])
    wait(rs2, ss.at[11])
    wait(back.at[pl.ds(0, NS - 1)], ss.at[12])


def local(dims, *args):
    NZ, NY, NX, TOK, LAT, D, WN, NN, NG = dims
    NT, NS = NY * NX, NZ * 2
    LT, LC, DC = TOK // NY, LAT // NX, D // NT
    CH = NZ // NG * LT
    HS = NS // NG
    ROWS = 2 * CAP * HS
    args = list(args)
    args[4] = args[4].reshape(1, -1)
    args[10] = args[10].reshape(1, -1)
    for i in (3, 11, 12, 13, 14, 16, 17):
        args[i] = jnp.swapaxes(args[i], -1, -2)
    FF = args[18].shape[0]
    args.append(jnp.asarray(rotary_table(NS * TOK)))
    shapes = [a.shape for a in args]
    shapes[9] = (TOK, DC)
    shapes[19] = (TOK, 2 * ROPE)
    shapes[13] = (2, 2, FF, D)
    shapes[16] = (2 * FF, D)
    kept = [i for i in range(20) if i not in (14, 17)]
    scratch = [pltpu.VMEM(shapes[i], args[i].dtype) for i in kept]
    scratch += [
        pltpu.VMEM((TOK, LAT), BF),
        pltpu.VMEM((LT, ROPE * NY), BF),
        pltpu.VMEM((NG, CH, LC), BF),
        pltpu.VMEM((LT, ROPE * NY), BF),
        pltpu.VMEM((2, NG, NY * CH, LAT), BF),
        pltpu.VMEM((2, NZ * LT, ROPE * NY), BF),
        pltpu.VMEM((2 * TOK, LAT), BF),
        pltpu.VMEM((2 * TOK, ROPE * NY), BF),
        pltpu.VMEM((2 * TOK, LAT), F32),
        pltpu.VMEM((TOK, D), BF),
        pltpu.VMEM((NT - 1, TOK, DC), BF),
        pltpu.VMEM((TOK, DC), BF),
        pltpu.VMEM((TOK, D), BF),
        pltpu.VMEM((TOK, D), BF),
        pltpu.VMEM((NT - 1, TOK, DC), BF),
        pltpu.VMEM((2, TOK, NS * SLOTS), BF),
        pltpu.VMEM((NS, SLOTS, DC), BF),
        pltpu.VMEM((NS, SLOTS, DC), BF),
        pltpu.VMEM((NG, ROWS, DC), BF),
        pltpu.VMEM((NG, ROWS, D), BF),
        pltpu.VMEM((NG, ROWS, D), BF),
        pltpu.VMEM((NG, NT - 1, ROWS, DC), BF),
        pltpu.VMEM((NG, HS, SLOTS, DC), BF),
        pltpu.VMEM((NS, SLOTS, DC), BF),
        pltpu.SemaphoreType.DMA((20,)),
        pltpu.SemaphoreType.DMA((13,)),
        pltpu.SemaphoreType.DMA((12,)),
        pltpu.SemaphoreType.DMA((NZ,)),
        pltpu.SemaphoreType.DMA((NZ,)),
        pltpu.SemaphoreType.DMA((NZ,)),
        pltpu.SemaphoreType.DMA((NG,)),
        pltpu.SemaphoreType.DMA((NG,)),
        pltpu.SemaphoreType.DMA((NT,)),
        pltpu.SemaphoreType.DMA((NG,)),
        pltpu.SemaphoreType.DMA((NG,)),
        pltpu.SemaphoreType.DMA((NG,)),
        pltpu.SemaphoreType.DMA((NG,)),
        pltpu.SemaphoreType.DMA((NG,)),
        pltpu.SemaphoreType.DMA((NG,)),
        pltpu.SemaphoreType.DMA((NG,)),
    ]
    return pl.pallas_call(
        functools.partial(kernel, dims),
        out_shape=pltpu.VMEM((TOK, DC), BF),
        in_specs=[pl.BlockSpec(memory_space=pltpu.HBM)] * 20,
        out_specs=pl.BlockSpec(memory_space=pltpu.VMEM),
        scratch_shapes=scratch,
        compiler_params=pltpu.CompilerParams(
            collective_id=0, has_side_effects=True, vmem_limit_bytes=60 * 1024 * 1024
        ),
        name="layer",
    )(*args)


def build(mesh, nz, ny, nx, tok, lat, d, wn, nn, ng):
    torus = Mesh(mesh.devices.reshape(nz, 2, ny, nx), ("z", "c", "y", "x"))
    SP, TP = ("z", "c"), ("y", "x")
    return jax.shard_map(
        functools.partial(local, (nz, ny, nx, tok, lat, d, wn, nn, ng)),
        mesh=torus,
        in_specs=(
            P(SP, TP),
            P(SP, TP),
            P(SP, None),
            P(SP, None),
            P(),
            P(None, TP),
            P(None, TP),
            P(TP, None),
            P(TP, None),
            P(SP, None),
            P(),
            P(SP, None),
            P(SP, None),
            P(SP, None, TP),
            P(SP, None, TP),
            P(SP, TP, None),
            P(None, TP),
            P(None, TP),
            P(TP, None),
        ),
        out_specs=P(SP, TP),
        check_vma=False,
    )


def solution(mesh):
    return build(mesh, 16, 4, 4, 64, 512, 2048, 128, 64, 4)
```

```python
import functools

import jax
import jax.numpy as jnp
import numpy as np
from jax import lax
from jax.experimental import pallas as pl
from jax.experimental.pallas import tpu as pltpu
from jax.sharding import Mesh
from jax.sharding import PartitionSpec as P

MESH = pl.DeviceIdType.MESH
ROPE = 32
CAP = 3
SLOTS = 8
THETA = 10000.0
EPS = 1e-06
FLOOR = -1e30
BF = jnp.bfloat16
F32 = jnp.float32


def rotary_table(tokens):
    half = ROPE // 2
    freq = np.float32(THETA) ** (-2.0 * np.arange(half, dtype=np.float32) / np.float32(ROPE))
    freq = freq.astype(np.float32)
    angles = np.arange(tokens, dtype=np.float32)[:, None] * freq[None, :]
    cosine = np.cos(angles.astype(np.float64)).astype(np.float32)
    sine = np.sin(angles.astype(np.float64)).astype(np.float32)
    return np.concatenate([cosine, cosine, -sine, sine], axis=1)


def dot(a, b, ca=1, cb=0):
    return lax.dot_general(a, b, (((ca,), (cb,)), ((), ())), preferred_element_type=F32)


def turned(values, table):
    half = ROPE // 2
    v = values.astype(F32)
    swapped = jnp.concatenate([v[:, half:], v[:, :half]], axis=1)
    return v * table[:, :ROPE] + swapped * table[:, ROPE : 2 * ROPE]


def normalized(values, gain):
    v = values.astype(F32)
    scaled = v * lax.rsqrt(jnp.mean(v * v, axis=-1, keepdims=True) + EPS)
    return (scaled * gain).astype(BF)


def eye(n):
    return lax.broadcasted_iota(jnp.int32, (n, n), 0) == lax.broadcasted_iota(jnp.int32, (n, n), 1)


def upright(line):
    return jnp.sum(jnp.where(eye(line.shape[1]), line, 0.0), axis=1, keepdims=True)


def silu(v):
    return v / (1.0 + jnp.exp(-v))


def shift_of(n):
    return n.bit_length() - 1


def kernel(dims, *refs):
    NZ, NY, NX, TOK, LAT, D, WN, NN, NG = dims
    NT, NS = NY * NX, NZ * 2
    LT, LC, DC = TOK // NY, LAT // NX, D // NT
    GZ = NZ // NG
    CH = GZ * LT
    KB = NY * CH
    HS = NS // NG
    Q = NS * SLOTS
    HQ = HS * SLOTS
    RPE = CAP * HS
    ROWS = 2 * RPE
    hbm, out_ref, scratch = refs[:20], refs[20], refs[21:]
    (
        v_wq, v_nq, v_lat, v_rk, v_lg, v_wkv, v_nkv, v_wo, v_no, v_res, v_ng, v_ids, v_rw,
        v_egu, v_ed, v_sgu, v_sd, v_tab,
        latn, rott, zbuf, zrot, lat_buf, rot_buf, qlat, qrp, mixd,
        pp, rsb, strm, sall, spp, shb, selt, disp, arr, xsend, xall, part, rs2, ret, back,
        lsem, ss, rs, zsem, zsend, rsend, psem, psend, qsem, csem, csend, dsem, dsend, asem, xsem, esem,
    ) = scratch
    FF = v_sd.shape[0]
    vmem = [
        v_wq, v_nq, v_lat, v_rk, v_lg, v_wkv, v_nkv, v_wo, v_no, v_res, v_ng, v_ids, v_rw,
        v_egu.at[0], v_egu.at[1], v_ed,
        v_sgu.at[pl.ds(0, FF)], v_sgu.at[pl.ds(FF, FF)], v_sd, v_tab,
    ]

    z, c = lax.axis_index("z"), lax.axis_index("c")
    y, x = lax.axis_index("y"), lax.axis_index("x")
    t = y * NX + x
    s = z * 2 + c
    gz = lax.div(z, GZ)

    def plane(k):
        t2 = lax.rem(t + k, NT)
        return {"y": lax.div(t2, NX), "x": lax.rem(t2, NX)}, t2

    def seq(k):
        s2 = lax.rem(s + k + NS // 4, NS)
        return {"z": lax.div(s2, 2), "c": lax.rem(s2, 2)}, s2

    def others(f):
        each(0, NS - NS // 4, f)
        each(NS - NS // 4 + 1, NS, f)

    def cols(i):
        return pl.ds(pl.multiple_of(i * DC, DC), DC)

    def send(src, dst, ssem, rsem, dev):
        pltpu.make_async_remote_copy(
            src_ref=src, dst_ref=dst, send_sem=ssem, recv_sem=rsem, device_id=dev, device_id_type=MESH
        ).start()

    def keep(src, dst, sem):
        pltpu.make_async_copy(src, dst, sem).start()

    def wait(ref, sem, name="w"):
        with jax.named_scope(name):
            pltpu.make_async_copy(ref, ref, sem).wait()

    def each(lo, hi, f):
        def body(k, carry):
            f(k)
            return carry

        lax.fori_loop(lo, hi, body, 0)

    bar = pltpu.get_barrier_semaphore()
    others(lambda k: pl.semaphore_signal(bar, inc=1, device_id=seq(k)[0], device_id_type=MESH))
    each(1, NT, lambda k: pl.semaphore_signal(bar, inc=1, device_id=plane(k)[0], device_id_type=MESH))

    loads = []
    for i in range(20):
        src = hbm[i]
        if i == 9:
            src = src.at[:, cols(t)]
        if i == 19:
            src = src.at[pl.ds(pl.multiple_of(s * TOK, TOK), TOK)]
        loads.append(pltpu.make_async_copy(src, vmem[i], lsem.at[i]))
    for i in (2, 3, 4, 19, 0, 1, 5, 6, 11, 12, 9, 7, 8, 10, 16, 17, 18, 13, 14, 15):
        loads[i].start()

    def loaded(*which):
        for i in which:
            loads[i].wait()

    def clear_tile(i):
        zbuf[gz, pl.ds(pl.multiple_of(i * LT, LT), LT)] = jnp.zeros((LT, LC), BF)

    def clear_turn(i):
        rot_buf[c, pl.ds(pl.multiple_of(i * LT, LT), LT)] = jnp.zeros((LT, ROPE * NY), BF)

    each(lax.rem(z, GZ) + 1, GZ, clear_tile)
    each(z + 1, NZ, clear_turn)

    loaded(2, 3, 4, 19)
    table = v_tab[...]
    latn[...] = normalized(v_lat[...], v_lg[...])
    rk = turned(dot(v_rk[...], eye(ROPE).astype(BF), 0, 0), table)
    rott[...] = jnp.concatenate([rk[i * LT : (i + 1) * LT] for i in range(NY)], axis=1).astype(BF)

    with jax.named_scope("w_bar"):
        pl.semaphore_wait(bar, NS + NT - 2)

    own_tile = latn.at[pl.ds(pl.multiple_of(y * LT, LT), LT), pl.ds(pl.multiple_of(x * LC, LC), LC)]
    zslot = zbuf.at[gz, pl.ds(pl.multiple_of(lax.rem(z, GZ) * LT, LT), LT)]

    each(1, NZ - z, lambda k: send(own_tile, zslot, zsend.at[k], zsem.at[z], {"z": z + k}))
    keep(own_tile, zslot, zsem.at[z])

    @pl.when(z == t)
    def _():
        each(1, NZ - z, lambda k: send(rott, zrot, rsend.at[k], rs.at[1], {"z": z + k}))
        keep(rott, zrot, rs.at[1])

    loaded(0, 1, 5, 6)
    wscale, nscale = (WN + ROPE) ** -0.5, (NN + ROPE) ** -0.5
    qlat[:TOK] = (dot(v_wq[:, :WN], v_wkv[:, :WN], 1, 1) * wscale).astype(BF)
    qlat[TOK:] = (dot(v_nq[:, :NN], v_nkv[:, :NN], 1, 1) * nscale).astype(BF)
    qr = jnp.concatenate(
        [turned(v_wq[:, WN:], table) * wscale, turned(v_nq[:, NN:], table) * nscale], axis=0
    )
    qrp[...] = jnp.concatenate([qr] * NY, axis=1).astype(BF)

    def lat_slot(g):
        return lat_buf.at[
            c, g, pl.ds(pl.multiple_of(y * CH, CH), CH), pl.ds(pl.multiple_of(x * LC, LC), LC)
        ]

    wrap = lax.div(z, NZ - 2) if NG > 2 else 0

    def group(k):
        first = lax.div(NG - k, NG)
        second = lax.div(NG + 1 - k, NG) - first
        top = lax.div(gz, NG - 1)
        near = lax.div(NG + 2 - k, NG) - first
        far_last = first * gz + near * (NG - 2) * (second * (1 - wrap) + (1 - second) * wrap) + (1 - first - near) * 1
        return top * far_last + (1 - top) * (gz - k) if NG > 2 else gz - k

    my_rot = rot_buf.at[c, pl.ds(pl.multiple_of(t * LT, LT), LT)]

    def tiles_of(g, k):
        lo = g * GZ
        whole = 1 - lax.div(NG - k, NG)
        return lo, lo + whole * GZ + (1 - whole) * (lax.rem(z, GZ) + 1)

    def group_out(k):
        g = group(k)
        each(*tiles_of(g, k), lambda i: wait(zslot, zsem.at[i], "w_z"))

        @pl.when((lax.div(t, GZ) == g) & (t <= z))
        def _():
            wait(zrot, rs.at[1], "w_zrot")
            keep(zrot, my_rot, qsem.at[t])
            each(1, NT, lambda i: send(zrot, my_rot, ss.at[3], qsem.at[t], plane(i)[0]))

        keep(zbuf.at[g], lat_slot(g), psem.at[g])
        each(1, NT, lambda i: send(zbuf.at[g], lat_slot(g), psend.at[g], psem.at[g], plane(i)[0]))

    each(0, gz + 1, group_out)

    loaded(11, 12)
    lane = lax.broadcasted_iota(jnp.int32, (TOK, Q), 1)
    j = lane & (SLOTS - 1)
    high = (j >= CAP).astype(jnp.int32)
    expert = ((lane >> shift_of(SLOTS)) * 2 + high).astype(F32)
    hit0 = upright(v_ids[0:1].astype(F32)) == expert
    hit1 = upright(v_ids[1:2].astype(F32)) == expert
    ahead = (
        lax.broadcasted_iota(jnp.int32, (TOK, TOK), 0) > lax.broadcasted_iota(jnp.int32, (TOK, TOK), 1)
    ).astype(F32)
    hits = jnp.where(hit0 | hit1, 1.0, 0.0).astype(F32)
    rank = dot(ahead.astype(BF), hits.astype(BF))
    fits = (rank == (j - CAP * high).astype(F32)) & (j < 2 * CAP)
    selt[0] = jnp.where(hit0 & fits, 1.0, 0.0).astype(BF)
    selt[1] = jnp.where(hit1 & fits, 1.0, 0.0).astype(BF)

    other = {"c": 1 - c}

    def turn_rows(p, g):
        return rot_buf.at[p, pl.ds(pl.multiple_of(g * CH, CH), CH)]

    def group_over(k):
        g = group(k)
        wait(lat_buf.at[c, g], psem.at[g], "w_plane")
        send(lat_buf.at[c, g], lat_buf.at[c, g], csend.at[g], csem.at[g], other)
        each(*tiles_of(g, k), lambda i: wait(zrot, qsem.at[i], "w_prot"))
        send(turn_rows(c, g), turn_rows(c, g), dsend.at[g], dsem.at[g], other)

    key = lax.broadcasted_iota(jnp.int32, (2 * TOK, KB), 1)
    key_at = (
        (key >> shift_of(CH)) * LT + ((key >> shift_of(LT)) & (GZ - 1)) * (2 * TOK) + (key & (LT - 1))
    )
    query_at = s * TOK + (lax.broadcasted_iota(jnp.int32, (2 * TOK, KB), 0) & (TOK - 1))
    ahead_by = query_at - key_at
    strip = lax.broadcasted_iota(jnp.int32, (CH, ROPE * NY), 1) >> shift_of(ROPE)
    mixd[...] = jnp.zeros_like(mixd)

    def attend(p, g, carry):
        peak, total = carry
        turns = rot_buf[p, pl.ds(pl.multiple_of(g * CH, CH), CH)].astype(F32)
        turns = jnp.concatenate([jnp.where(strip == i, turns, 0.0) for i in range(NY)], axis=0)
        keys = lat_buf[p, g]
        scores = dot(qlat[...], keys, 1, 1) + dot(qrp[...], turns.astype(BF), 1, 1)
        scores = jnp.where(ahead_by >= p * TOK + g * (GZ * 2 * TOK), scores, FLOOR)
        newest = jnp.maximum(peak, jnp.max(scores, axis=-1, keepdims=True))
        fade = jnp.exp(peak - newest)
        probs = jnp.exp(scores - newest)
        mixd[...] = mixd[...] * fade + dot(probs.astype(BF), keys)
        return newest, total * fade + jnp.sum(probs, axis=-1, keepdims=True)

    def other_attend(k, carry):
        g = group(k)
        wait(lat_buf.at[1 - c, g], csem.at[g], "w_core")
        wait(turn_rows(1 - c, g), dsem.at[g], "w_crot")
        return attend(1 - c, g, carry)

    def both_attend(k, carry):
        group_over(k)
        carry = attend(c, group(k), carry)
        return lax.fori_loop(jnp.maximum(k - 1, 0), k, other_attend, carry)

    carry = (jnp.full((2 * TOK, 1), FLOOR, F32), jnp.zeros((2 * TOK, 1), F32))
    carry = lax.fori_loop(0, gz + 1, both_attend, carry)
    _, total = lax.fori_loop(gz, gz + 1, other_attend, carry)
    mixed = (mixd[...] / total).astype(BF)
    wide = dot(mixed[:TOK], v_wkv[:, WN:]).astype(BF)
    narrow = dot(mixed[TOK:], v_nkv[...])[:, NN:].astype(BF)
    loaded(7, 8, 9)
    pp[...] = (dot(wide, v_wo[...]) + dot(narrow, v_no[...])).astype(BF)

    late = z >= GZ

    def spread(rows, slots, r_axis):
        row = lax.broadcasted_iota(jnp.int32, (rows, slots), r_axis)
        slot = lax.broadcasted_iota(jnp.int32, (rows, slots), 1 - r_axis)
        return jnp.where(slot == (row & (HS - 1)) * SLOTS + (row >> shift_of(HS)), 1.0, 0.0).astype(BF)

    def rows_out(h):
        wait(arr.at[pl.ds(h * HS, HS)], asem.at[h], f"w_arr{h}")
        came = arr[h * HS : (h + 1) * HS].astype(F32).reshape(HQ, DC).astype(BF)
        xsend[h] = dot(spread(ROWS, HQ, 0), came).astype(BF)
        each(1, NT, lambda k: send(xsend.at[h], xall.at[h, :, cols(t)], ss.at[10], xsem.at[h], plane(k)[0]))
        keep(xsend.at[h], xall.at[h, :, cols(t)], xsem.at[h])

    def experts(h):
        wait(xall.at[h], xsem.at[h], f"w_xall{h}")
        both = dot(normalized(xall[h], v_ng[...]), v_egu[...].reshape(4 * FF, D), 1, 1)
        hidden = silu(both[:, : 2 * FF]) * both[:, 2 * FF :]
        first = lax.broadcasted_iota(jnp.int32, (ROWS, 2 * FF), 0) < RPE
        hidden = jnp.where(first == (lax.broadcasted_iota(jnp.int32, (ROWS, 2 * FF), 1) < FF), hidden, 0.0)
        part[h] = dot(hidden.astype(BF), v_ed[...].reshape(2 * FF, D)).astype(BF)

        def e_send(k):
            dev, t2 = plane(k)
            send(part.at[h, :, cols(t2)], rs2.at[h, k - 1], ss.at[11], esem.at[h], dev)

        each(1, NT, e_send)

    def rows_back(h):
        acc = part[h, :, cols(t)].astype(F32)
        wait(rs2.at[h], esem.at[h], f"w_rs2_{h}")
        for k in range(NT - 1):
            acc = acc + rs2[h, k].astype(F32)
        ret[h] = dot(spread(HQ, ROWS, 1), acc.astype(BF)).reshape(HS, SLOTS, DC).astype(BF)

        def b_send(k):
            r2 = lax.rem(s + k, HS)
            s2 = h * HS + r2

            @pl.when(s2 != s)
            def _():
                send(ret.at[h, r2], back.at[s], ss.at[12], rs.at[11], {"z": lax.div(s2, 2), "c": lax.rem(s2, 2)})

            @pl.when(s2 == s)
            def _():
                keep(ret.at[h, r2], back.at[s], rs.at[11])

        each(0, HS, b_send)

    def pp_send(k):
        dev, t2 = plane(k)
        send(pp.at[:, cols(t2)], rsb.at[k - 1], ss.at[6], rs.at[5], dev)

    each(1, NT, pp_send)
    loaded(10, 16, 17, 18, 13, 14, 15)
    acc = pp[:, cols(t)].astype(F32)
    wait(rsb, rs.at[5], "w_proj")
    for k in range(NT - 1):
        acc = acc + rsb[k].astype(F32)
    stream = (v_res[...].astype(F32) + acc.astype(BF).astype(F32)).astype(BF)
    strm[...] = stream

    bunch = lax.div(s, HS)
    disp[...] = dot(selt[0] + selt[1], stream, 0, 0).reshape(NS, SLOTS, DC).astype(BF)

    def d_send(k):
        dev, s2 = seq(k)
        send(disp.at[s2], arr.at[s], ss.at[7], asem.at[bunch], dev)

    others(d_send)
    keep(disp.at[s], arr.at[s], asem.at[bunch])

    def stream_out():
        each(1, NT, lambda k: send(strm, sall.at[:, cols(t)], ss.at[8], rs.at[7], plane(k)[0]))
        keep(strm, sall.at[:, cols(t)], rs.at[7])

    def shared_expert():
        wait(sall, rs.at[7], "w_sall")
        both = dot(normalized(sall[...], v_ng[...]), v_sgu[...], 1, 1)
        hidden = (silu(both[:, :FF]) * both[:, FF:]).astype(BF)
        spp[...] = dot(hidden, v_sd[...]).astype(BF)

    def shared_out():
        def sh_send(k):
            dev, t2 = plane(k)
            send(spp.at[:, cols(t2)], shb.at[k - 1], ss.at[9], rs.at[8], dev)

        each(1, NT, sh_send)

    @pl.when(jnp.logical_not(late))
    def _():
        stream_out()
        shared_expert()
        rows_out(0)
        shared_out()

    @pl.when(late)
    def _():
        rows_out(0)
        stream_out()

    rows_out(1)
    experts(0)
    for h in range(2, NG):
        rows_out(h)
    for h in range(1, NG - 1):
        experts(h)
        if h == 1:
            rows_back(0)

    @pl.when(late)
    def _():
        shared_expert()

    experts(NG - 1)

    @pl.when(late)
    def _():
        shared_out()

    for h in range(1 if NG > 2 else 0, NG):
        rows_back(h)

    shared = spp[:, cols(t)].astype(F32)
    wait(shb, rs.at[8], "w_shb")
    for k in range(NT - 1):
        shared = shared + shb[k].astype(F32)
    before = strm[...].astype(F32) + shared.astype(BF).astype(F32)

    wait(back, rs.at[11], "w_back")
    rows = back[...].astype(F32).reshape(Q, DC).astype(BF)
    routed = dot(selt[0], rows) * upright(v_rw[0:1]) + dot(selt[1], rows) * upright(v_rw[1:2])
    out_ref[...] = (before + routed).astype(BF)

    each(1, NZ - z, lambda k: wait(zslot, zsend.at[k]))

    @pl.when(z == t)
    def _():
        each(1, NZ - z, lambda k: wait(zrot, rsend.at[k]))

    each(0, gz + 1, lambda g: wait(lat_buf.at[0, 0, pl.ds(0, KB * (NT - 1) // NT)], psend.at[g]))

    @pl.when(t <= z)
    def _():
        wait(rot_buf.at[0, pl.ds(0, (NT - 1) * LT)], ss.at[3])

    each(0, gz + 1, lambda g: wait(lat_buf.at[0, 0], csend.at[g]))
    each(0, gz + 1, lambda g: wait(turn_rows(0, 0), dsend.at[g]))
    wait(rsb, ss.at[6])
    wait(disp.at[pl.ds(0, NS - 1)], ss.at[7])
    wait(rsb, ss.at[8])
    wait(shb, ss.at[9])
    wait(rs2, ss.at[10])
    wait(rs2, ss.at[11])
    wait(back.at[pl.ds(0, NS - 1)], ss.at[12])


def local(dims, *args):
    NZ, NY, NX, TOK, LAT, D, WN, NN, NG = dims
    NT, NS = NY * NX, NZ * 2
    LT, LC, DC = TOK // NY, LAT // NX, D // NT
    CH = NZ // NG * LT
    HS = NS // NG
    ROWS = 2 * CAP * HS
    args = list(args)
    args[4] = args[4].reshape(1, -1)
    args[10] = args[10].reshape(1, -1)
    for i in (3, 11, 12, 13, 14, 16, 17):
        args[i] = jnp.swapaxes(args[i], -1, -2)
    FF = args[18].shape[0]
    args.append(jnp.asarray(rotary_table(NS * TOK)))
    shapes = [a.shape for a in args]
    shapes[9] = (TOK, DC)
    shapes[19] = (TOK, 2 * ROPE)
    shapes[13] = (2, 2, FF, D)
    shapes[16] = (2 * FF, D)
    kept = [i for i in range(20) if i not in (14, 17)]
    scratch = [pltpu.VMEM(shapes[i], args[i].dtype) for i in kept]
    scratch += [
        pltpu.VMEM((TOK, LAT), BF),
        pltpu.VMEM((LT, ROPE * NY), BF),
        pltpu.VMEM((NG, CH, LC), BF),
        pltpu.VMEM((LT, ROPE * NY), BF),
        pltpu.VMEM((2, NG, NY * CH, LAT), BF),
        pltpu.VMEM((2, NZ * LT, ROPE * NY), BF),
        pltpu.VMEM((2 * TOK, LAT), BF),
        pltpu.VMEM((2 * TOK, ROPE * NY), BF),
        pltpu.VMEM((2 * TOK, LAT), F32),
        pltpu.VMEM((TOK, D), BF),
        pltpu.VMEM((NT - 1, TOK, DC), BF),
        pltpu.VMEM((TOK, DC), BF),
        pltpu.VMEM((TOK, D), BF),
        pltpu.VMEM((TOK, D), BF),
        pltpu.VMEM((NT - 1, TOK, DC), BF),
        pltpu.VMEM((2, TOK, NS * SLOTS), BF),
        pltpu.VMEM((NS, SLOTS, DC), BF),
        pltpu.VMEM((NS, SLOTS, DC), BF),
        pltpu.VMEM((NG, ROWS, DC), BF),
        pltpu.VMEM((NG, ROWS, D), BF),
        pltpu.VMEM((NG, ROWS, D), BF),
        pltpu.VMEM((NG, NT - 1, ROWS, DC), BF),
        pltpu.VMEM((NG, HS, SLOTS, DC), BF),
        pltpu.VMEM((NS, SLOTS, DC), BF),
        pltpu.SemaphoreType.DMA((20,)),
        pltpu.SemaphoreType.DMA((13,)),
        pltpu.SemaphoreType.DMA((12,)),
        pltpu.SemaphoreType.DMA((NZ,)),
        pltpu.SemaphoreType.DMA((NZ,)),
        pltpu.SemaphoreType.DMA((NZ,)),
        pltpu.SemaphoreType.DMA((NG,)),
        pltpu.SemaphoreType.DMA((NG,)),
        pltpu.SemaphoreType.DMA((NT,)),
        pltpu.SemaphoreType.DMA((NG,)),
        pltpu.SemaphoreType.DMA((NG,)),
        pltpu.SemaphoreType.DMA((NG,)),
        pltpu.SemaphoreType.DMA((NG,)),
        pltpu.SemaphoreType.DMA((NG,)),
        pltpu.SemaphoreType.DMA((NG,)),
        pltpu.SemaphoreType.DMA((NG,)),
    ]
    return pl.pallas_call(
        functools.partial(kernel, dims),
        out_shape=pltpu.VMEM((TOK, DC), BF),
        in_specs=[pl.BlockSpec(memory_space=pltpu.HBM)] * 20,
        out_specs=pl.BlockSpec(memory_space=pltpu.VMEM),
        scratch_shapes=scratch,
        compiler_params=pltpu.CompilerParams(
            collective_id=0, has_side_effects=True, vmem_limit_bytes=60 * 1024 * 1024
        ),
        name="layer",
    )(*args)


def build(mesh, nz, ny, nx, tok, lat, d, wn, nn, ng):
    torus = Mesh(mesh.devices.reshape(nz, 2, ny, nx), ("z", "c", "y", "x"))
    SP, TP = ("z", "c"), ("y", "x")
    return jax.shard_map(
        functools.partial(local, (nz, ny, nx, tok, lat, d, wn, nn, ng)),
        mesh=torus,
        in_specs=(
            P(SP, TP),
            P(SP, TP),
            P(SP, None),
            P(SP, None),
            P(),
            P(None, TP),
            P(None, TP),
            P(TP, None),
            P(TP, None),
            P(SP, None),
            P(),
            P(SP, None),
            P(SP, None),
            P(SP, None, TP),
            P(SP, None, TP),
            P(SP, TP, None),
            P(None, TP),
            P(None, TP),
            P(TP, None),
        ),
        out_specs=P(SP, TP),
        check_vma=False,
    )


def solution(mesh):
    return build(mesh, 16, 4, 4, 64, 512, 2048, 128, 64, 4)
```

```python
import functools

import jax
import jax.numpy as jnp
import numpy as np
from jax import lax
from jax.experimental import pallas as pl
from jax.experimental.pallas import tpu as pltpu
from jax.sharding import Mesh
from jax.sharding import PartitionSpec as P

MESH = pl.DeviceIdType.MESH
ROPE = 32
CAP = 3
SLOTS = 8
THETA = 10000.0
EPS = 1e-06
FLOOR = -1e30
BF = jnp.bfloat16
F32 = jnp.float32


def rotary_table(tokens):
    half = ROPE // 2
    freq = np.float32(THETA) ** (-2.0 * np.arange(half, dtype=np.float32) / np.float32(ROPE))
    freq = freq.astype(np.float32)
    angles = np.arange(tokens, dtype=np.float32)[:, None] * freq[None, :]
    cosine = np.cos(angles.astype(np.float64)).astype(np.float32)
    sine = np.sin(angles.astype(np.float64)).astype(np.float32)
    return np.concatenate([cosine, cosine, -sine, sine], axis=1)


def dot(a, b, ca=1, cb=0):
    return lax.dot_general(a, b, (((ca,), (cb,)), ((), ())), preferred_element_type=F32)


def turned(values, table):
    half = ROPE // 2
    v = values.astype(F32)
    swapped = jnp.concatenate([v[:, half:], v[:, :half]], axis=1)
    return v * table[:, :ROPE] + swapped * table[:, ROPE : 2 * ROPE]


def normalized(values, gain):
    v = values.astype(F32)
    scaled = v * lax.rsqrt(jnp.mean(v * v, axis=-1, keepdims=True) + EPS)
    return (scaled * gain).astype(BF)


def eye(n):
    return lax.broadcasted_iota(jnp.int32, (n, n), 0) == lax.broadcasted_iota(jnp.int32, (n, n), 1)


def upright(line):
    return jnp.sum(jnp.where(eye(line.shape[1]), line, 0.0), axis=1, keepdims=True)


def silu(v):
    return v / (1.0 + jnp.exp(-v))


def shift_of(n):
    return n.bit_length() - 1


def kernel(dims, *refs):
    NZ, NY, NX, TOK, LAT, D, WN, NN, NG = dims
    NT, NS = NY * NX, NZ * 2
    LT, LC, DC = TOK // NY, LAT // NX, D // NT
    GZ = NZ // NG
    CH = GZ * LT
    KB = NY * CH
    HS = NS // NG
    Q = NS * SLOTS
    HQ = HS * SLOTS
    RPE = CAP * HS
    ROWS = 2 * RPE
    hbm, out_ref, scratch = refs[:20], refs[20], refs[21:]
    (
        v_wq, v_nq, v_lat, v_rk, v_lg, v_wkv, v_nkv, v_wno, v_res, v_ng, v_ids, v_rw,
        v_egu, v_ed, v_sgu, v_sd, v_tab,
        latn, rott, zbuf, zrot, lat_buf, rot_buf, qlat, qrp, mixd,
        pp, rsb, strm, sall, spp, shb, selt, disp, arr, xsend, xall, part, rs2, ret, back,
        lsem, ss, rs, zsem, zsend, rsend, psem, psend, qsem, csem, csend, dsem, dsend, tsem, tsend, asem, xsem, esem,
    ) = scratch
    FF = v_sd.shape[0]
    WV, NV = hbm[7].shape[0], hbm[8].shape[0]
    vmem = [
        v_wq, v_nq, v_lat, v_rk, v_lg, v_wkv, v_nkv, v_wno.at[pl.ds(0, WV)], v_wno.at[pl.ds(WV, NV)],
        v_res, v_ng, v_ids, v_rw,
        v_egu.at[0], v_egu.at[1], v_ed,
        v_sgu.at[pl.ds(0, FF)], v_sgu.at[pl.ds(FF, FF)], v_sd, v_tab,
    ]

    z, c = lax.axis_index("z"), lax.axis_index("c")
    y, x = lax.axis_index("y"), lax.axis_index("x")
    t = y * NX + x
    s = z * 2 + c
    gz = lax.div(z, GZ)

    def plane(k):
        t2 = lax.rem(t + k, NT)
        return {"y": lax.div(t2, NX), "x": lax.rem(t2, NX)}, t2

    def seq(k):
        s2 = lax.rem(s + k + NS // 4, NS)
        return {"z": lax.div(s2, 2), "c": lax.rem(s2, 2)}, s2

    def others(f):
        each(0, NS - NS // 4, f)
        each(NS - NS // 4 + 1, NS, f)

    def cols(i):
        return pl.ds(pl.multiple_of(i * DC, DC), DC)

    def send(src, dst, ssem, rsem, dev):
        pltpu.make_async_remote_copy(
            src_ref=src, dst_ref=dst, send_sem=ssem, recv_sem=rsem, device_id=dev, device_id_type=MESH
        ).start()

    def keep(src, dst, sem):
        pltpu.make_async_copy(src, dst, sem).start()

    def wait(ref, sem, name="w"):
        with jax.named_scope(name):
            pltpu.make_async_copy(ref, ref, sem).wait()

    def each(lo, hi, f):
        def body(k, carry):
            f(k)
            return carry

        lax.fori_loop(lo, hi, body, 0)

    bar = pltpu.get_barrier_semaphore()
    others(lambda k: pl.semaphore_signal(bar, inc=1, device_id=seq(k)[0], device_id_type=MESH))
    each(1, NT, lambda k: pl.semaphore_signal(bar, inc=1, device_id=plane(k)[0], device_id_type=MESH))

    loads = []
    for i in range(20):
        src = hbm[i]
        if i == 9:
            src = src.at[:, cols(t)]
        if i == 19:
            src = src.at[pl.ds(pl.multiple_of(s * TOK, TOK), TOK)]
        loads.append(pltpu.make_async_copy(src, vmem[i], lsem.at[i]))
    for i in (2, 3, 4, 19, 0, 1, 5, 6, 11, 12, 9, 7, 8, 10, 16, 17, 18, 13, 14, 15):
        loads[i].start()

    def loaded(*which):
        for i in which:
            loads[i].wait()

    def clear_tile(i):
        zbuf[gz, pl.ds(pl.multiple_of(i * LT, LT), LT)] = jnp.zeros((LT, LC), BF)

    def clear_turn(i):
        rot_buf[c, pl.ds(pl.multiple_of(i * LT, LT), LT)] = jnp.zeros((LT, ROPE * NY), BF)

    each(lax.rem(z, GZ) + 1, GZ, clear_tile)
    each(z + 1, NZ, clear_turn)

    loaded(2, 3, 4, 19)
    table = v_tab[...]
    latn[...] = normalized(v_lat[...], v_lg[...])
    rk = turned(dot(v_rk[...], eye(ROPE).astype(BF), 0, 0), table)
    rott[...] = jnp.concatenate([rk[i * LT : (i + 1) * LT] for i in range(NY)], axis=1).astype(BF)

    with jax.named_scope("w_bar"):
        pl.semaphore_wait(bar, NS + NT - 2)

    own_tile = latn.at[pl.ds(pl.multiple_of(y * LT, LT), LT), pl.ds(pl.multiple_of(x * LC, LC), LC)]
    zslot = zbuf.at[gz, pl.ds(pl.multiple_of(lax.rem(z, GZ) * LT, LT), LT)]

    each(1, NZ - z, lambda k: send(own_tile, zslot, zsend.at[k], zsem.at[z], {"z": z + k}))
    keep(own_tile, zslot, zsem.at[z])

    @pl.when(z == t)
    def _():
        each(1, NZ - z, lambda k: send(rott, zrot, rsend.at[k], rs.at[1], {"z": z + k}))
        keep(rott, zrot, rs.at[1])

    loaded(0, 1, 5, 6)
    wscale, nscale = (WN + ROPE) ** -0.5, (NN + ROPE) ** -0.5
    qlat[:TOK] = (dot(v_wq[:, :WN], v_wkv[:, :WN], 1, 1) * wscale).astype(BF)
    qlat[TOK:] = (dot(v_nq[:, :NN], v_nkv[:, :NN], 1, 1) * nscale).astype(BF)
    qr = jnp.concatenate(
        [turned(v_wq[:, WN:], table) * wscale, turned(v_nq[:, NN:], table) * nscale], axis=0
    )
    qrp[...] = jnp.concatenate([qr] * NY, axis=1).astype(BF)

    def lat_slot(g):
        return lat_buf.at[c, g, y, :, x_cols]

    x_cols = pl.ds(pl.multiple_of(x * LC, LC), LC)
    HC = CH // 2
    half = (pl.ds(0, HC), pl.ds(HC, HC))
    two = lax.div(gz, NG - 1)

    def along_x(f):
        each(1, NX, lambda k: f({"x": lax.rem(x + k, NX)}))

    def along_y(f):
        each(1, NY, lambda k: f({"y": lax.rem(y + k, NY)}))

    def group_on(k):
        g = group(k)
        row = lat_buf.at[c, g, y, half[0], :]
        wait(row, tsem.at[0, g], "w_step")
        along_y(lambda dev: send(row, row, tsend.at[2, g], tsem.at[2, g], dev))
        column = lat_buf.at[c, g, :, half[1], x_cols]
        wait(column, tsem.at[1, g], "w_step")
        along_x(lambda dev: send(column, column, tsend.at[3, g], tsem.at[3, g], dev))

    wrap = lax.div(z, NZ - 2) if NG > 2 else 0

    def group(k):
        first = lax.div(NG - k, NG)
        second = lax.div(NG + 1 - k, NG) - first
        top = lax.div(gz, NG - 1)
        near = lax.div(NG + 2 - k, NG) - first
        far_last = first * gz + near * (NG - 2) * (second * (1 - wrap) + (1 - second) * wrap) + (1 - first - near) * 1
        return top * far_last + (1 - top) * (gz - k) if NG > 2 else gz - k

    my_rot = rot_buf.at[c, pl.ds(pl.multiple_of(t * LT, LT), LT)]

    def tiles_of(g, k):
        lo = g * GZ
        whole = 1 - lax.div(NG - k, NG)
        return lo, lo + whole * GZ + (1 - whole) * (lax.rem(z, GZ) + 1)

    def group_out(k):
        g = group(k)
        each(*tiles_of(g, k), lambda i: wait(zslot, zsem.at[i], "w_z"))

        @pl.when((lax.div(t, GZ) == g) & (t <= z))
        def _():
            wait(zrot, rs.at[1], "w_zrot")
            keep(zrot, my_rot, qsem.at[t])
            each(1, NT, lambda i: send(zrot, my_rot, ss.at[3], qsem.at[t], plane(i)[0]))

        @pl.when(two == 0)
        def _():
            keep(zbuf.at[g], lat_slot(g), psem.at[g])
            each(1, NT, lambda i: send(zbuf.at[g], lat_slot(g), psend.at[g], psem.at[g], plane(i)[0]))

        @pl.when(two == 1)
        def _():
            for i, along in ((0, along_x), (1, along_y)):
                src, dst = zbuf.at[g, half[i]], lat_buf.at[c, g, y, half[i], x_cols]
                keep(src, dst, tsem.at[i, g])
                along(lambda dev, src=src, dst=dst, i=i: send(src, dst, tsend.at[i, g], tsem.at[i, g], dev))

    each(0, 1, group_out)

    @pl.when(two == 1)
    def _():
        each(0, 1, group_on)

    each(1, gz + 1, group_out)

    @pl.when(two == 1)
    def _():
        each(1, gz + 1, group_on)

    loaded(11, 12)
    lane = lax.broadcasted_iota(jnp.int32, (TOK, Q), 1)
    j = lane & (SLOTS - 1)
    high = (j >= CAP).astype(jnp.int32)
    expert = ((lane >> shift_of(SLOTS)) * 2 + high).astype(F32)
    hit0 = upright(v_ids[0:1].astype(F32)) == expert
    hit1 = upright(v_ids[1:2].astype(F32)) == expert
    ahead = (
        lax.broadcasted_iota(jnp.int32, (TOK, TOK), 0) > lax.broadcasted_iota(jnp.int32, (TOK, TOK), 1)
    ).astype(F32)
    hits = jnp.where(hit0 | hit1, 1.0, 0.0).astype(F32)
    rank = dot(ahead.astype(BF), hits.astype(BF))
    fits = (rank == (j - CAP * high).astype(F32)) & (j < 2 * CAP)
    selt[0] = jnp.where(hit0 & fits, 1.0, 0.0).astype(BF)
    selt[1] = jnp.where(hit1 & fits, 1.0, 0.0).astype(BF)

    other = {"c": 1 - c}

    def turn_rows(p, g):
        return rot_buf.at[p, pl.ds(pl.multiple_of(g * CH, CH), CH)]

    def group_over(k):
        g = group(k)

        @pl.when(two == 0)
        def _():
            wait(lat_buf.at[c, g], psem.at[g], "w_plane")

        @pl.when(two == 1)
        def _():
            wait(lat_buf.at[c, g, pl.ds(0, NY - 1), half[0], :], tsem.at[2, g], "w_plane")
            wait(lat_buf.at[c, g, :, half[1], pl.ds(0, (NX - 1) * LC)], tsem.at[3, g], "w_plane")

        send(lat_buf.at[c, g], lat_buf.at[c, g], csend.at[g], csem.at[g], other)
        each(*tiles_of(g, k), lambda i: wait(zrot, qsem.at[i], "w_prot"))
        send(turn_rows(c, g), turn_rows(c, g), dsend.at[g], dsem.at[g], other)

    key = lax.broadcasted_iota(jnp.int32, (2 * TOK, KB), 1)
    key_at = (
        (key >> shift_of(CH)) * LT + ((key >> shift_of(LT)) & (GZ - 1)) * (2 * TOK) + (key & (LT - 1))
    )
    query_at = s * TOK + (lax.broadcasted_iota(jnp.int32, (2 * TOK, KB), 0) & (TOK - 1))
    ahead_by = query_at - key_at
    strip = lax.broadcasted_iota(jnp.int32, (CH, ROPE * NY), 1) >> shift_of(ROPE)
    mixd[...] = jnp.zeros_like(mixd)

    def scored(p, g):
        turns = rot_buf[p, pl.ds(pl.multiple_of(g * CH, CH), CH)].astype(F32)
        turns = jnp.concatenate([jnp.where(strip == i, turns, 0.0) for i in range(NY)], axis=0)
        keys = lat_buf[p, g].reshape(KB, LAT)
        scores = dot(qlat[...], keys, 1, 1) + dot(qrp[...], turns.astype(BF), 1, 1)
        return jnp.where(ahead_by >= p * TOK + g * (GZ * 2 * TOK), scores, FLOOR)

    def attend(places, carry):
        peak, total = carry
        scores = [scored(p, g) for p, g in places]
        newest = peak
        for sc in scores:
            newest = jnp.maximum(newest, jnp.max(sc, axis=-1, keepdims=True))
        fade = jnp.exp(peak - newest)
        mixed, total = mixd[...] * fade, total * fade
        for (p, g), sc in zip(places, scores):
            probs = jnp.exp(sc - newest)
            total = total + jnp.sum(probs, axis=-1, keepdims=True)
            mixed = mixed + dot(probs.astype(BF), lat_buf[p, g].reshape(KB, LAT))
        mixd[...] = mixed
        return newest, total

    def wait_other(k):
        g = group(k)
        wait(lat_buf.at[1 - c, g], csem.at[g], "w_core")
        wait(turn_rows(1 - c, g), dsem.at[g], "w_crot")

    def both_attend(k, carry):
        group_over(k)
        wait_other(k - 1)
        return attend([(c, group(k)), (1 - c, group(k - 1))], carry)

    carry = (jnp.full((2 * TOK, 1), FLOOR, F32), jnp.zeros((2 * TOK, 1), F32))
    group_over(0)
    carry = attend([(c, gz)], carry)
    carry = lax.fori_loop(1, gz + 1, both_attend, carry)
    wait_other(gz)
    _, total = attend([(1 - c, group(gz))], carry)
    mixed = (mixd[...] / total).astype(BF)
    wide = dot(mixed[:TOK], v_wkv[:, WN:])
    narrow = dot(mixed[TOK:], v_nkv[...])[:, NN:]
    loaded(7, 8, 9)
    pp[...] = dot(jnp.concatenate([wide, narrow], axis=1).astype(BF), v_wno[...]).astype(BF)

    late = z >= GZ

    def spread(rows, slots, r_axis):
        row = lax.broadcasted_iota(jnp.int32, (rows, slots), r_axis)
        slot = lax.broadcasted_iota(jnp.int32, (rows, slots), 1 - r_axis)
        return jnp.where(slot == (row & (HS - 1)) * SLOTS + (row >> shift_of(HS)), 1.0, 0.0).astype(BF)

    def rows_out(h):
        wait(arr.at[pl.ds(h * HS, HS)], asem.at[h], f"w_arr{h}")
        came = arr[h * HS : (h + 1) * HS].astype(F32).reshape(HQ, DC).astype(BF)
        xsend[h] = dot(spread(ROWS, HQ, 0), came).astype(BF)
        each(1, NT, lambda k: send(xsend.at[h], xall.at[h, :, cols(t)], ss.at[10], xsem.at[h], plane(k)[0]))
        keep(xsend.at[h], xall.at[h, :, cols(t)], xsem.at[h])

    def experts(h):
        wait(xall.at[h], xsem.at[h], f"w_xall{h}")
        both = dot(normalized(xall[h], v_ng[...]), v_egu[...].reshape(4 * FF, D), 1, 1)
        hidden = silu(both[:, : 2 * FF]) * both[:, 2 * FF :]
        first = lax.broadcasted_iota(jnp.int32, (ROWS, 2 * FF), 0) < RPE
        hidden = jnp.where(first == (lax.broadcasted_iota(jnp.int32, (ROWS, 2 * FF), 1) < FF), hidden, 0.0)
        part[h] = dot(hidden.astype(BF), v_ed[...].reshape(2 * FF, D)).astype(BF)

        def e_send(k):
            dev, t2 = plane(k)
            send(part.at[h, :, cols(t2)], rs2.at[h, k - 1], ss.at[11], esem.at[h], dev)

        each(1, NT, e_send)

    def rows_back(h):
        acc = part[h, :, cols(t)].astype(F32)
        wait(rs2.at[h], esem.at[h], f"w_rs2_{h}")
        for k in range(NT - 1):
            acc = acc + rs2[h, k].astype(F32)
        ret[h] = dot(spread(HQ, ROWS, 1), acc.astype(BF)).reshape(HS, SLOTS, DC).astype(BF)

        def b_send(k):
            r2 = lax.rem(s + k, HS)
            s2 = h * HS + r2

            @pl.when(s2 != s)
            def _():
                send(ret.at[h, r2], back.at[s], ss.at[12], rs.at[11], {"z": lax.div(s2, 2), "c": lax.rem(s2, 2)})

            @pl.when(s2 == s)
            def _():
                keep(ret.at[h, r2], back.at[s], rs.at[11])

        each(0, HS, b_send)

    def pp_send(k):
        dev, t2 = plane(k)
        send(pp.at[:, cols(t2)], rsb.at[k - 1], ss.at[6], rs.at[5], dev)

    each(1, NT, pp_send)
    loaded(10, 16, 17, 18, 13, 14, 15)
    acc = pp[:, cols(t)].astype(F32)
    wait(rsb, rs.at[5], "w_proj")
    for k in range(NT - 1):
        acc = acc + rsb[k].astype(F32)
    stream = (v_res[...].astype(F32) + acc.astype(BF).astype(F32)).astype(BF)
    strm[...] = stream

    bunch = lax.div(s, HS)
    disp[...] = dot(selt[0] + selt[1], stream, 0, 0).reshape(NS, SLOTS, DC).astype(BF)

    def d_send(k):
        dev, s2 = seq(k)
        send(disp.at[s2], arr.at[s], ss.at[7], asem.at[bunch], dev)

    others(d_send)
    keep(disp.at[s], arr.at[s], asem.at[bunch])

    def stream_out():
        each(1, NT, lambda k: send(strm, sall.at[:, cols(t)], ss.at[8], rs.at[7], plane(k)[0]))
        keep(strm, sall.at[:, cols(t)], rs.at[7])

    def shared_expert():
        wait(sall, rs.at[7], "w_sall")
        both = dot(normalized(sall[...], v_ng[...]), v_sgu[...], 1, 1)
        hidden = (silu(both[:, :FF]) * both[:, FF:]).astype(BF)
        spp[...] = dot(hidden, v_sd[...]).astype(BF)

    def shared_out():
        def sh_send(k):
            dev, t2 = plane(k)
            send(spp.at[:, cols(t2)], shb.at[k - 1], ss.at[9], rs.at[8], dev)

        each(1, NT, sh_send)

    @pl.when(jnp.logical_not(late))
    def _():
        stream_out()
        rows_out(0)
        shared_expert()
        shared_out()

    @pl.when(late)
    def _():
        rows_out(0)
        stream_out()

    rows_out(1)
    experts(0)
    for h in range(2, NG):
        rows_out(h)
    for h in range(1, NG - 1):
        experts(h)
        if h == 1:
            rows_back(0)
    experts(NG - 1)
    for h in range(1 if NG > 2 else 0, NG - 1):
        rows_back(h)

    @pl.when(late)
    def _():
        shared_expert()
        shared_out()

    rows_back(NG - 1)

    each(1, NZ - z, lambda k: wait(zslot, zsend.at[k]))

    @pl.when(z == t)
    def _():
        each(1, NZ - z, lambda k: wait(zrot, rsend.at[k]))

    chunks = rsb if CH * LC == TOK * DC else lat_buf.at[0, 0, :, pl.ds(0, CH * (NT - 1) // NT)]

    @pl.when(two == 0)
    def _():
        each(0, gz + 1, lambda g: wait(chunks, psend.at[g]))

    @pl.when(two == 1)
    def _():
        def left(g):
            wait(lat_buf.at[0, 0, 0, half[0], pl.ds(0, (NX - 1) * LC)], tsend.at[0, g])
            wait(lat_buf.at[0, 0, pl.ds(0, NY - 1), half[0], pl.ds(0, LC)], tsend.at[1, g])
            wait(lat_buf.at[0, 0, pl.ds(0, NY - 1), half[0], :], tsend.at[2, g])
            wait(lat_buf.at[0, 0, :, half[0], pl.ds(0, (NX - 1) * LC)], tsend.at[3, g])

        each(0, gz + 1, left)

    @pl.when(t <= z)
    def _():
        wait(rot_buf.at[0, pl.ds(0, (NT - 1) * LT)], ss.at[3])

    each(0, gz + 1, lambda g: wait(lat_buf.at[0, 0], csend.at[g]))
    each(0, gz + 1, lambda g: wait(turn_rows(0, 0), dsend.at[g]))
    wait(rsb, ss.at[6])
    wait(disp.at[pl.ds(0, NS - 1)], ss.at[7])
    wait(rsb, ss.at[8])
    wait(rs2, ss.at[10])
    wait(rs2, ss.at[11])

    first_weight, second_weight = upright(v_rw[0:1]), upright(v_rw[1:2])
    shared = spp[:, cols(t)].astype(F32)
    wait(shb, rs.at[8], "w_shb")
    for k in range(NT - 1):
        shared = shared + shb[k].astype(F32)
    before = strm[...].astype(F32) + shared.astype(BF).astype(F32)

    wait(back, rs.at[11], "w_back")
    rows = back[...].astype(F32).reshape(Q, DC).astype(BF)
    routed = dot(selt[0], rows) * first_weight + dot(selt[1], rows) * second_weight
    out_ref[...] = (before + routed).astype(BF)
    wait(shb, ss.at[9])
    wait(back.at[pl.ds(0, NS - 1)], ss.at[12])


def local(dims, *args):
    NZ, NY, NX, TOK, LAT, D, WN, NN, NG = dims
    NT, NS = NY * NX, NZ * 2
    LT, LC, DC = TOK // NY, LAT // NX, D // NT
    CH = NZ // NG * LT
    HS = NS // NG
    ROWS = 2 * CAP * HS
    args = list(args)
    args[4] = args[4].reshape(1, -1)
    args[10] = args[10].reshape(1, -1)
    for i in (3, 11, 12, 13, 14, 16, 17):
        args[i] = jnp.swapaxes(args[i], -1, -2)
    FF = args[18].shape[0]
    args.append(jnp.asarray(rotary_table(NS * TOK)))
    shapes = [a.shape for a in args]
    shapes[9] = (TOK, DC)
    shapes[19] = (TOK, 2 * ROPE)
    shapes[13] = (2, 2, FF, D)
    shapes[16] = (2 * FF, D)
    shapes[7] = (shapes[7][0] + shapes[8][0], D)
    kept = [i for i in range(20) if i not in (8, 14, 17)]
    scratch = [pltpu.VMEM(shapes[i], args[i].dtype) for i in kept]
    scratch += [
        pltpu.VMEM((TOK, LAT), BF),
        pltpu.VMEM((LT, ROPE * NY), BF),
        pltpu.VMEM((NG, CH, LC), BF),
        pltpu.VMEM((LT, ROPE * NY), BF),
        pltpu.VMEM((2, NG, NY, CH, LAT), BF),
        pltpu.VMEM((2, NZ * LT, ROPE * NY), BF),
        pltpu.VMEM((2 * TOK, LAT), BF),
        pltpu.VMEM((2 * TOK, ROPE * NY), BF),
        pltpu.VMEM((2 * TOK, LAT), F32),
        pltpu.VMEM((TOK, D), BF),
        pltpu.VMEM((NT - 1, TOK, DC), BF),
        pltpu.VMEM((TOK, DC), BF),
        pltpu.VMEM((TOK, D), BF),
        pltpu.VMEM((TOK, D), BF),
        pltpu.VMEM((NT - 1, TOK, DC), BF),
        pltpu.VMEM((2, TOK, NS * SLOTS), BF),
        pltpu.VMEM((NS, SLOTS, DC), BF),
        pltpu.VMEM((NS, SLOTS, DC), BF),
        pltpu.VMEM((NG, ROWS, DC), BF),
        pltpu.VMEM((NG, ROWS, D), BF),
        pltpu.VMEM((NG, ROWS, D), BF),
        pltpu.VMEM((NG, NT - 1, ROWS, DC), BF),
        pltpu.VMEM((NG, HS, SLOTS, DC), BF),
        pltpu.VMEM((NS, SLOTS, DC), BF),
        pltpu.SemaphoreType.DMA((20,)),
        pltpu.SemaphoreType.DMA((13,)),
        pltpu.SemaphoreType.DMA((12,)),
        pltpu.SemaphoreType.DMA((NZ,)),
        pltpu.SemaphoreType.DMA((NZ,)),
        pltpu.SemaphoreType.DMA((NZ,)),
        pltpu.SemaphoreType.DMA((NG,)),
        pltpu.SemaphoreType.DMA((NG,)),
        pltpu.SemaphoreType.DMA((NT,)),
        pltpu.SemaphoreType.DMA((NG,)),
        pltpu.SemaphoreType.DMA((NG,)),
        pltpu.SemaphoreType.DMA((NG,)),
        pltpu.SemaphoreType.DMA((NG,)),
        pltpu.SemaphoreType.DMA((4, NG)),
        pltpu.SemaphoreType.DMA((4, NG)),
        pltpu.SemaphoreType.DMA((NG,)),
        pltpu.SemaphoreType.DMA((NG,)),
        pltpu.SemaphoreType.DMA((NG,)),
    ]
    return pl.pallas_call(
        functools.partial(kernel, dims),
        out_shape=pltpu.VMEM((TOK, DC), BF),
        in_specs=[pl.BlockSpec(memory_space=pltpu.HBM)] * 20,
        out_specs=pl.BlockSpec(memory_space=pltpu.VMEM),
        scratch_shapes=scratch,
        compiler_params=pltpu.CompilerParams(
            collective_id=0, has_side_effects=True, vmem_limit_bytes=60 * 1024 * 1024
        ),
        name="layer",
    )(*args)


def build(mesh, nz, ny, nx, tok, lat, d, wn, nn, ng):
    torus = Mesh(mesh.devices.reshape(nz, 2, ny, nx), ("z", "c", "y", "x"))
    SP, TP = ("z", "c"), ("y", "x")
    return jax.shard_map(
        functools.partial(local, (nz, ny, nx, tok, lat, d, wn, nn, ng)),
        mesh=torus,
        in_specs=(
            P(SP, TP),
            P(SP, TP),
            P(SP, None),
            P(SP, None),
            P(),
            P(None, TP),
            P(None, TP),
            P(TP, None),
            P(TP, None),
            P(SP, None),
            P(),
            P(SP, None),
            P(SP, None),
            P(SP, None, TP),
            P(SP, None, TP),
            P(SP, TP, None),
            P(None, TP),
            P(None, TP),
            P(TP, None),
        ),
        out_specs=P(SP, TP),
        check_vma=False,
    )


def solution(mesh):
    return build(mesh, 16, 4, 4, 64, 512, 2048, 128, 64, 4)
```

```python
import functools

import jax
import jax.numpy as jnp
import numpy as np
from jax import lax
from jax.experimental import pallas as pl
from jax.experimental.pallas import tpu as pltpu
from jax.sharding import Mesh
from jax.sharding import PartitionSpec as P

MESH = pl.DeviceIdType.MESH
ROPE = 32
CAP = 3
SLOTS = 8
THETA = 10000.0
EPS = 1e-06
FLOOR = -1e30
BF = jnp.bfloat16
F32 = jnp.float32


def rotary_table(tokens):
    half = ROPE // 2
    freq = np.float32(THETA) ** (-2.0 * np.arange(half, dtype=np.float32) / np.float32(ROPE))
    freq = freq.astype(np.float32)
    angles = np.arange(tokens, dtype=np.float32)[:, None] * freq[None, :]
    cosine = np.cos(angles.astype(np.float64)).astype(np.float32)
    sine = np.sin(angles.astype(np.float64)).astype(np.float32)
    return np.concatenate([cosine, cosine, -sine, sine], axis=1)


def dot(a, b, ca=1, cb=0):
    return lax.dot_general(a, b, (((ca,), (cb,)), ((), ())), preferred_element_type=F32)


def turned(values, table):
    half = ROPE // 2
    v = values.astype(F32)
    swapped = jnp.concatenate([v[:, half:], v[:, :half]], axis=1)
    return v * table[:, :ROPE] + swapped * table[:, ROPE : 2 * ROPE]


def normalized(values, gain):
    v = values.astype(F32)
    scaled = v * lax.rsqrt(jnp.mean(v * v, axis=-1, keepdims=True) + EPS)
    return (scaled * gain).astype(BF)


def eye(n):
    return lax.broadcasted_iota(jnp.int32, (n, n), 0) == lax.broadcasted_iota(jnp.int32, (n, n), 1)


def upright(line):
    return jnp.sum(jnp.where(eye(line.shape[1]), line, 0.0), axis=1, keepdims=True)


def silu(v):
    return v / (1.0 + jnp.exp(-v))


def shift_of(n):
    return n.bit_length() - 1


def kernel(dims, *refs):
    NZ, NY, NX, TOK, LAT, D, WN, NN, NG = dims
    NT, NS = NY * NX, NZ * 2
    LT, LC, DC = TOK // NY, LAT // NX, D // NT
    GZ = NZ // NG
    CH = GZ * LT
    KB = NY * CH
    HS = NS // NG
    Q = NS * SLOTS
    HQ = HS * SLOTS
    RPE = CAP * HS
    ROWS = 2 * RPE
    hbm, out_ref, scratch = refs[:20], refs[20], refs[21:]
    (
        v_wq, v_nq, v_lat, v_rk, v_lg, v_wkv, v_nkv, v_wno, v_res, v_ng, v_ids, v_rw,
        v_egu, v_ed, v_sgu, v_sd, v_tab,
        latn, rott, zbuf, zrot, lat_buf, rot_buf, qlat, qrp, mixd,
        pp, rsb, strm, sall, spp, shb, selt, disp, arr, xsend, xall, part, rs2, ret, back, v_wt,
        lsem, ss, rs, zsem, zsend, rsend, psem, psend, qsem, csem, csend, dsem, dsend, tsem, tsend, asem, xsem, esem,
    ) = scratch
    FF = v_sd.shape[0]
    WV, NV = hbm[7].shape[0], hbm[8].shape[0]
    vmem = [
        v_wq, v_nq, v_lat, v_rk, v_lg, v_wkv, v_nkv, v_wno.at[pl.ds(0, WV)], v_wno.at[pl.ds(WV, NV)],
        v_res, v_ng, v_ids, v_rw,
        v_egu.at[0], v_egu.at[1], v_ed,
        v_sgu.at[pl.ds(0, FF)], v_sgu.at[pl.ds(FF, FF)], v_sd, v_tab,
    ]

    z, c = lax.axis_index("z"), lax.axis_index("c")
    y, x = lax.axis_index("y"), lax.axis_index("x")
    t = y * NX + x
    s = z * 2 + c
    gz = lax.div(z, GZ)

    def plane(k):
        t2 = lax.rem(t + k, NT)
        return {"y": lax.div(t2, NX), "x": lax.rem(t2, NX)}, t2

    def seq(k):
        s2 = lax.rem(s + k + NS // 4, NS)
        return {"z": lax.div(s2, 2), "c": lax.rem(s2, 2)}, s2

    def others(f):
        each(0, NS - NS // 4, f)
        each(NS - NS // 4 + 1, NS, f)

    def cols(i):
        return pl.ds(pl.multiple_of(i * DC, DC), DC)

    def send(src, dst, ssem, rsem, dev):
        pltpu.make_async_remote_copy(
            src_ref=src, dst_ref=dst, send_sem=ssem, recv_sem=rsem, device_id=dev, device_id_type=MESH
        ).start()

    def keep(src, dst, sem):
        pltpu.make_async_copy(src, dst, sem).start()

    def wait(ref, sem, name="w"):
        with jax.named_scope(name):
            pltpu.make_async_copy(ref, ref, sem).wait()

    def each(lo, hi, f):
        run = 1
        if isinstance(lo, int) and isinstance(hi, int):
            run = max([u for u in range(1, 8) if (hi - lo) % u == 0], default=1)

        def body(k, carry):
            for i in range(run):
                f(lo + k * run + i if run > 1 else k)
            return carry

        if run > 1:
            lax.fori_loop(0, (hi - lo) // run, body, 0)
        else:
            lax.fori_loop(lo, hi, body, 0)

    bar = pltpu.get_barrier_semaphore()
    others(lambda k: pl.semaphore_signal(bar, inc=1, device_id=seq(k)[0], device_id_type=MESH))
    each(1, NT, lambda k: pl.semaphore_signal(bar, inc=1, device_id=plane(k)[0], device_id_type=MESH))

    loads = []
    for i in range(20):
        src = hbm[i]
        if i == 9:
            src = src.at[:, cols(t)]
        if i == 19:
            src = src.at[pl.ds(pl.multiple_of(s * TOK, TOK), TOK)]
        loads.append(pltpu.make_async_copy(src, vmem[i], lsem.at[i]))
    for i in (2, 3, 4, 19, 0, 1, 5, 6, 11, 12, 9, 7, 8, 10, 16, 17, 18, 13, 14, 15):
        loads[i].start()

    def loaded(*which):
        for i in which:
            loads[i].wait()

    def clear_tile(i):
        zbuf[gz, pl.ds(pl.multiple_of(i * LT, LT), LT)] = jnp.zeros((LT, LC), BF)

    def clear_turn(i):
        rot_buf[c, pl.ds(pl.multiple_of(i * LT, LT), LT)] = jnp.zeros((LT, ROPE * NY), BF)

    each(lax.rem(z, GZ) + 1, GZ, clear_tile)
    each(z + 1, NZ, clear_turn)

    loaded(2, 3, 4, 19)
    table = v_tab[...]
    latn[...] = normalized(v_lat[...], v_lg[...])
    rk = turned(dot(v_rk[...], eye(ROPE).astype(BF), 0, 0), table)
    rott[...] = jnp.concatenate([rk[i * LT : (i + 1) * LT] for i in range(NY)], axis=1).astype(BF)

    with jax.named_scope("w_bar"):
        pl.semaphore_wait(bar, NS + NT - 2)

    own_tile = latn.at[pl.ds(pl.multiple_of(y * LT, LT), LT), pl.ds(pl.multiple_of(x * LC, LC), LC)]
    zslot = zbuf.at[gz, pl.ds(pl.multiple_of(lax.rem(z, GZ) * LT, LT), LT)]

    each(1, NZ - z, lambda k: send(own_tile, zslot, zsend.at[k], zsem.at[z], {"z": z + k}))
    keep(own_tile, zslot, zsem.at[z])

    @pl.when(z == t)
    def _():
        each(1, NZ - z, lambda k: send(rott, zrot, rsend.at[k], rs.at[1], {"z": z + k}))
        keep(rott, zrot, rs.at[1])

    loaded(0, 1, 5, 6)
    wscale, nscale = (WN + ROPE) ** -0.5, (NN + ROPE) ** -0.5
    qlat[:TOK] = (dot(v_wq[:, :WN], v_wkv[:, :WN], 1, 1) * wscale).astype(BF)
    qlat[TOK:] = (dot(v_nq[:, :NN], v_nkv[:, :NN], 1, 1) * nscale).astype(BF)
    qr = jnp.concatenate(
        [turned(v_wq[:, WN:], table) * wscale, turned(v_nq[:, NN:], table) * nscale], axis=0
    )
    qrp[...] = jnp.concatenate([qr] * NY, axis=1).astype(BF)

    def lat_slot(g):
        return lat_buf.at[c, g, y, :, x_cols]

    x_cols = pl.ds(pl.multiple_of(x * LC, LC), LC)
    HC = CH // 2
    half = (pl.ds(0, HC), pl.ds(HC, HC))
    two = lax.div(gz, NG - 1)

    def along_x(f):
        each(1, NX, lambda k: f({"x": lax.rem(x + k, NX)}))

    def along_y(f):
        each(1, NY, lambda k: f({"y": lax.rem(y + k, NY)}))

    def group_on(k):
        g = group(k)
        row = lat_buf.at[c, g, y, half[0], :]
        wait(row, tsem.at[0, g], "w_step")
        along_y(lambda dev: send(row, row, tsend.at[2, g], tsem.at[2, g], dev))
        column = lat_buf.at[c, g, :, half[1], x_cols]
        wait(column, tsem.at[1, g], "w_step")
        along_x(lambda dev: send(column, column, tsend.at[3, g], tsem.at[3, g], dev))

    wrap = lax.div(z, NZ - 2) if NG > 2 else 0

    def group(k):
        first = lax.div(NG - k, NG)
        second = lax.div(NG + 1 - k, NG) - first
        top = lax.div(gz, NG - 1)
        near = lax.div(NG + 2 - k, NG) - first
        far_last = first * gz + near * (NG - 2) * (second * (1 - wrap) + (1 - second) * wrap) + (1 - first - near) * 1
        return top * far_last + (1 - top) * (gz - k) if NG > 2 else gz - k

    my_rot = rot_buf.at[c, pl.ds(pl.multiple_of(t * LT, LT), LT)]

    def tiles_of(g, k):
        lo = g * GZ
        whole = 1 - lax.div(NG - k, NG)
        return lo, lo + whole * GZ + (1 - whole) * (lax.rem(z, GZ) + 1)

    def group_out(k):
        g = group(k)
        each(*tiles_of(g, k), lambda i: wait(zslot, zsem.at[i], "w_z"))

        @pl.when((lax.div(t, GZ) == g) & (t <= z))
        def _():
            wait(zrot, rs.at[1], "w_zrot")
            keep(zrot, my_rot, qsem.at[t])
            each(1, NT, lambda i: send(zrot, my_rot, ss.at[3], qsem.at[t], plane(i)[0]))

        @pl.when(two == 0)
        def _():
            keep(zbuf.at[g], lat_slot(g), psem.at[g])
            each(1, NT, lambda i: send(zbuf.at[g], lat_slot(g), psend.at[g], psem.at[g], plane(i)[0]))

        @pl.when(two == 1)
        def _():
            for i, along in ((0, along_x), (1, along_y)):
                src, dst = zbuf.at[g, half[i]], lat_buf.at[c, g, y, half[i], x_cols]
                keep(src, dst, tsem.at[i, g])
                along(lambda dev, src=src, dst=dst, i=i: send(src, dst, tsend.at[i, g], tsem.at[i, g], dev))

    each(0, 1, group_out)

    @pl.when(two == 1)
    def _():
        each(0, 1, group_on)

    each(1, gz + 1, group_out)

    @pl.when(two == 1)
    def _():
        each(1, gz + 1, group_on)

    loaded(11, 12)
    lane = lax.broadcasted_iota(jnp.int32, (TOK, Q), 1)
    j = lane & (SLOTS - 1)
    high = (j >= CAP).astype(jnp.int32)
    expert = ((lane >> shift_of(SLOTS)) * 2 + high).astype(F32)
    hit0 = upright(v_ids[0:1].astype(F32)) == expert
    hit1 = upright(v_ids[1:2].astype(F32)) == expert
    ahead = (
        lax.broadcasted_iota(jnp.int32, (TOK, TOK), 0) > lax.broadcasted_iota(jnp.int32, (TOK, TOK), 1)
    ).astype(F32)
    hits = jnp.where(hit0 | hit1, 1.0, 0.0).astype(F32)
    rank = dot(ahead.astype(BF), hits.astype(BF))
    fits = (rank == (j - CAP * high).astype(F32)) & (j < 2 * CAP)
    selt[0] = jnp.where(hit0 & fits, 1.0, 0.0).astype(BF)
    selt[1] = jnp.where(hit1 & fits, 1.0, 0.0).astype(BF)

    other = {"c": 1 - c}

    def turn_rows(p, g):
        return rot_buf.at[p, pl.ds(pl.multiple_of(g * CH, CH), CH)]

    def group_over(k):
        g = group(k)

        @pl.when(two == 0)
        def _():
            wait(lat_buf.at[c, g], psem.at[g], "w_plane")

        @pl.when(two == 1)
        def _():
            wait(lat_buf.at[c, g, pl.ds(0, NY - 1), half[0], :], tsem.at[2, g], "w_plane")
            wait(lat_buf.at[c, g, :, half[1], pl.ds(0, (NX - 1) * LC)], tsem.at[3, g], "w_plane")

        send(lat_buf.at[c, g], lat_buf.at[c, g], csend.at[g], csem.at[g], other)
        each(*tiles_of(g, k), lambda i: wait(zrot, qsem.at[i], "w_prot"))
        send(turn_rows(c, g), turn_rows(c, g), dsend.at[g], dsem.at[g], other)

    key = lax.broadcasted_iota(jnp.int32, (2 * TOK, KB), 1)
    key_at = (
        (key >> shift_of(CH)) * LT + ((key >> shift_of(LT)) & (GZ - 1)) * (2 * TOK) + (key & (LT - 1))
    )
    query_at = s * TOK + (lax.broadcasted_iota(jnp.int32, (2 * TOK, KB), 0) & (TOK - 1))
    ahead_by = query_at - key_at
    strip = lax.broadcasted_iota(jnp.int32, (CH, ROPE * NY), 1) >> shift_of(ROPE)
    mixd[...] = jnp.zeros_like(mixd)

    def scored(p, g):
        turns = rot_buf[p, pl.ds(pl.multiple_of(g * CH, CH), CH)].astype(F32)
        turns = jnp.concatenate([jnp.where(strip == i, turns, 0.0) for i in range(NY)], axis=0)
        keys = lat_buf[p, g].reshape(KB, LAT)
        scores = dot(qlat[...], keys, 1, 1) + dot(qrp[...], turns.astype(BF), 1, 1)
        return jnp.where(ahead_by >= p * TOK + g * (GZ * 2 * TOK), scores, FLOOR)

    def attend(places, carry):
        peak, total = carry
        scores = [scored(p, g) for p, g in places]
        newest = peak
        for sc in scores:
            newest = jnp.maximum(newest, jnp.max(sc, axis=-1, keepdims=True))
        fade = jnp.exp(peak - newest)
        mixed, total = mixd[...] * fade, total * fade
        for (p, g), sc in zip(places, scores):
            probs = jnp.exp(sc - newest)
            total = total + jnp.sum(probs, axis=-1, keepdims=True)
            mixed = mixed + dot(probs.astype(BF), lat_buf[p, g].reshape(KB, LAT))
        mixd[...] = mixed
        return newest, total

    def wait_other(k):
        g = group(k)
        wait(lat_buf.at[1 - c, g], csem.at[g], "w_core")
        wait(turn_rows(1 - c, g), dsem.at[g], "w_crot")

    def both_attend(k, carry):
        group_over(k)
        wait_other(k - 1)
        return attend([(c, group(k)), (1 - c, group(k - 1))], carry)

    carry = (jnp.full((2 * TOK, 1), FLOOR, F32), jnp.zeros((2 * TOK, 1), F32))
    group_over(0)
    carry = attend([(c, gz)], carry)
    carry = lax.fori_loop(1, gz + 1, both_attend, carry)
    wait_other(gz)
    _, total = attend([(1 - c, group(gz))], carry)
    mixed = (mixd[...] / total).astype(BF)
    wide = dot(mixed[:TOK], v_wkv[:, WN:])
    narrow = dot(mixed[TOK:], v_nkv[...])[:, NN:]
    loaded(7, 8, 9)
    pp[...] = dot(jnp.concatenate([wide, narrow], axis=1).astype(BF), v_wno[...]).astype(BF)

    late = z >= GZ

    def spread(rows, slots, r_axis):
        row = lax.broadcasted_iota(jnp.int32, (rows, slots), r_axis)
        slot = lax.broadcasted_iota(jnp.int32, (rows, slots), 1 - r_axis)
        return jnp.where(slot == (row & (HS - 1)) * SLOTS + (row >> shift_of(HS)), 1.0, 0.0).astype(BF)

    def rows_out(h):
        wait(arr.at[pl.ds(h * HS, HS)], asem.at[h], f"w_arr{h}")
        came = arr[h * HS : (h + 1) * HS].astype(F32).reshape(HQ, DC).astype(BF)
        xsend[h] = dot(spread(ROWS, HQ, 0), came).astype(BF)
        each(1, NT, lambda k: send(xsend.at[h], xall.at[h, :, cols(t)], ss.at[10], xsem.at[h], plane(k)[0]))
        keep(xsend.at[h], xall.at[h, :, cols(t)], xsem.at[h])

    def experts(h):
        wait(xall.at[h], xsem.at[h], f"w_xall{h}")
        both = dot(normalized(xall[h], v_ng[...]), v_wt[...])
        hidden = silu(both[:, : 2 * FF]) * both[:, 2 * FF :]
        first = lax.broadcasted_iota(jnp.int32, (ROWS, 2 * FF), 0) < RPE
        hidden = jnp.where(first == (lax.broadcasted_iota(jnp.int32, (ROWS, 2 * FF), 1) < FF), hidden, 0.0)
        part[h] = dot(hidden.astype(BF), v_ed[...].reshape(2 * FF, D)).astype(BF)

        def e_send(k):
            dev, t2 = plane(k)
            send(part.at[h, :, cols(t2)], rs2.at[h, k - 1], ss.at[11], esem.at[h], dev)

        each(1, NT, e_send)

    def rows_back(h):
        acc = part[h, :, cols(t)].astype(F32)
        wait(rs2.at[h], esem.at[h], f"w_rs2_{h}")
        for k in range(NT - 1):
            acc = acc + rs2[h, k].astype(F32)
        ret[h] = dot(spread(HQ, ROWS, 1), acc.astype(BF)).reshape(HS, SLOTS, DC).astype(BF)

        def b_send(k):
            r2 = lax.rem(s + k, HS)
            s2 = h * HS + r2

            @pl.when(s2 != s)
            def _():
                send(ret.at[h, r2], back.at[s], ss.at[12], rs.at[11], {"z": lax.div(s2, 2), "c": lax.rem(s2, 2)})

            @pl.when(s2 == s)
            def _():
                keep(ret.at[h, r2], back.at[s], rs.at[11])

        each(0, HS, b_send)

    def pp_send(k):
        dev, t2 = plane(k)
        send(pp.at[:, cols(t2)], rsb.at[k - 1], ss.at[6], rs.at[5], dev)

    each(1, NT, pp_send)
    loaded(10, 16, 17, 18, 13, 14, 15)
    v_wt[...] = v_egu[...].reshape(4 * FF, D).T
    acc = pp[:, cols(t)].astype(F32)
    wait(rsb, rs.at[5], "w_proj")
    for k in range(NT - 1):
        acc = acc + rsb[k].astype(F32)
    stream = (v_res[...].astype(F32) + acc.astype(BF).astype(F32)).astype(BF)
    strm[...] = stream

    bunch = lax.div(s, HS)
    disp[...] = dot(selt[0] + selt[1], stream, 0, 0).reshape(NS, SLOTS, DC).astype(BF)

    def d_send(k):
        dev, s2 = seq(k)
        send(disp.at[s2], arr.at[s], ss.at[7], asem.at[bunch], dev)

    others(d_send)
    keep(disp.at[s], arr.at[s], asem.at[bunch])

    def stream_out():
        each(1, NT, lambda k: send(strm, sall.at[:, cols(t)], ss.at[8], rs.at[7], plane(k)[0]))
        keep(strm, sall.at[:, cols(t)], rs.at[7])

    def shared_expert():
        wait(sall, rs.at[7], "w_sall")
        both = dot(normalized(sall[...], v_ng[...]), v_sgu[...], 1, 1)
        hidden = (silu(both[:, :FF]) * both[:, FF:]).astype(BF)
        spp[...] = dot(hidden, v_sd[...]).astype(BF)

    def shared_out():
        def sh_send(k):
            dev, t2 = plane(k)
            send(spp.at[:, cols(t2)], shb.at[k - 1], ss.at[9], rs.at[8], dev)

        each(1, NT, sh_send)

    @pl.when(jnp.logical_not(late))
    def _():
        stream_out()
        rows_out(0)
        shared_expert()
        shared_out()

    @pl.when(late)
    def _():
        rows_out(0)
        stream_out()

    rows_out(1)
    experts(0)
    for h in range(2, NG):
        rows_out(h)
    for h in range(1, NG - 1):
        experts(h)
        if h == 1:
            rows_back(0)
    experts(NG - 1)
    for h in range(1 if NG > 2 else 0, NG - 1):
        rows_back(h)

    @pl.when(late)
    def _():
        shared_expert()
        shared_out()

    rows_back(NG - 1)

    each(1, NZ - z, lambda k: wait(zslot, zsend.at[k]))

    @pl.when(z == t)
    def _():
        each(1, NZ - z, lambda k: wait(zrot, rsend.at[k]))

    chunks = rsb if CH * LC == TOK * DC else lat_buf.at[0, 0, :, pl.ds(0, CH * (NT - 1) // NT)]

    @pl.when(two == 0)
    def _():
        each(0, gz + 1, lambda g: wait(chunks, psend.at[g]))

    @pl.when(two == 1)
    def _():
        def left(g):
            wait(lat_buf.at[0, 0, 0, half[0], pl.ds(0, (NX - 1) * LC)], tsend.at[0, g])
            wait(lat_buf.at[0, 0, pl.ds(0, NY - 1), half[0], pl.ds(0, LC)], tsend.at[1, g])
            wait(lat_buf.at[0, 0, pl.ds(0, NY - 1), half[0], :], tsend.at[2, g])
            wait(lat_buf.at[0, 0, :, half[0], pl.ds(0, (NX - 1) * LC)], tsend.at[3, g])

        each(0, gz + 1, left)

    @pl.when(t <= z)
    def _():
        wait(rot_buf.at[0, pl.ds(0, (NT - 1) * LT)], ss.at[3])

    each(0, gz + 1, lambda g: wait(lat_buf.at[0, 0], csend.at[g]))
    each(0, gz + 1, lambda g: wait(turn_rows(0, 0), dsend.at[g]))
    wait(rsb, ss.at[6])
    wait(disp.at[pl.ds(0, NS - 1)], ss.at[7])
    wait(rsb, ss.at[8])
    wait(rs2, ss.at[10])
    wait(rs2, ss.at[11])

    first_weight, second_weight = upright(v_rw[0:1]), upright(v_rw[1:2])
    shared = spp[:, cols(t)].astype(F32)
    wait(shb, rs.at[8], "w_shb")
    for k in range(NT - 1):
        shared = shared + shb[k].astype(F32)
    before = strm[...].astype(F32) + shared.astype(BF).astype(F32)

    wait(back, rs.at[11], "w_back")
    rows = back[...].astype(F32).reshape(Q, DC).astype(BF)
    picked = dot(selt[...].reshape(2 * TOK, Q), rows)
    routed = picked[:TOK] * first_weight + picked[TOK:] * second_weight
    out_ref[...] = (before + routed).astype(BF)
    wait(shb, ss.at[9])
    wait(back.at[pl.ds(0, NS - 1)], ss.at[12])


def local(dims, *args):
    NZ, NY, NX, TOK, LAT, D, WN, NN, NG = dims
    NT, NS = NY * NX, NZ * 2
    LT, LC, DC = TOK // NY, LAT // NX, D // NT
    CH = NZ // NG * LT
    HS = NS // NG
    ROWS = 2 * CAP * HS
    args = list(args)
    args[4] = args[4].reshape(1, -1)
    args[10] = args[10].reshape(1, -1)
    for i in (3, 11, 12, 13, 14, 16, 17):
        args[i] = jnp.swapaxes(args[i], -1, -2)
    FF = args[18].shape[0]
    args.append(jnp.asarray(rotary_table(NS * TOK)))
    shapes = [a.shape for a in args]
    shapes[9] = (TOK, DC)
    shapes[19] = (TOK, 2 * ROPE)
    shapes[13] = (2, 2, FF, D)
    shapes[16] = (2 * FF, D)
    shapes[7] = (shapes[7][0] + shapes[8][0], D)
    kept = [i for i in range(20) if i not in (8, 14, 17)]
    scratch = [pltpu.VMEM(shapes[i], args[i].dtype) for i in kept]
    scratch += [
        pltpu.VMEM((TOK, LAT), BF),
        pltpu.VMEM((LT, ROPE * NY), BF),
        pltpu.VMEM((NG, CH, LC), BF),
        pltpu.VMEM((LT, ROPE * NY), BF),
        pltpu.VMEM((2, NG, NY, CH, LAT), BF),
        pltpu.VMEM((2, NZ * LT, ROPE * NY), BF),
        pltpu.VMEM((2 * TOK, LAT), BF),
        pltpu.VMEM((2 * TOK, ROPE * NY), BF),
        pltpu.VMEM((2 * TOK, LAT), F32),
        pltpu.VMEM((TOK, D), BF),
        pltpu.VMEM((NT - 1, TOK, DC), BF),
        pltpu.VMEM((TOK, DC), BF),
        pltpu.VMEM((TOK, D), BF),
        pltpu.VMEM((TOK, D), BF),
        pltpu.VMEM((NT - 1, TOK, DC), BF),
        pltpu.VMEM((2, TOK, NS * SLOTS), BF),
        pltpu.VMEM((NS, SLOTS, DC), BF),
        pltpu.VMEM((NS, SLOTS, DC), BF),
        pltpu.VMEM((NG, ROWS, DC), BF),
        pltpu.VMEM((NG, ROWS, D), BF),
        pltpu.VMEM((NG, ROWS, D), BF),
        pltpu.VMEM((NG, NT - 1, ROWS, DC), BF),
        pltpu.VMEM((NG, HS, SLOTS, DC), BF),
        pltpu.VMEM((NS, SLOTS, DC), BF),
        pltpu.VMEM((D, 4 * FF), BF),
        pltpu.SemaphoreType.DMA((20,)),
        pltpu.SemaphoreType.DMA((13,)),
        pltpu.SemaphoreType.DMA((12,)),
        pltpu.SemaphoreType.DMA((NZ,)),
        pltpu.SemaphoreType.DMA((NZ,)),
        pltpu.SemaphoreType.DMA((NZ,)),
        pltpu.SemaphoreType.DMA((NG,)),
        pltpu.SemaphoreType.DMA((NG,)),
        pltpu.SemaphoreType.DMA((NT,)),
        pltpu.SemaphoreType.DMA((NG,)),
        pltpu.SemaphoreType.DMA((NG,)),
        pltpu.SemaphoreType.DMA((NG,)),
        pltpu.SemaphoreType.DMA((NG,)),
        pltpu.SemaphoreType.DMA((4, NG)),
        pltpu.SemaphoreType.DMA((4, NG)),
        pltpu.SemaphoreType.DMA((NG,)),
        pltpu.SemaphoreType.DMA((NG,)),
        pltpu.SemaphoreType.DMA((NG,)),
    ]
    return pl.pallas_call(
        functools.partial(kernel, dims),
        out_shape=pltpu.VMEM((TOK, DC), BF),
        in_specs=[pl.BlockSpec(memory_space=pltpu.HBM)] * 20,
        out_specs=pl.BlockSpec(memory_space=pltpu.VMEM),
        scratch_shapes=scratch,
        compiler_params=pltpu.CompilerParams(
            collective_id=0, has_side_effects=True, vmem_limit_bytes=60 * 1024 * 1024
        ),
        name="layer",
    )(*args)


def build(mesh, nz, ny, nx, tok, lat, d, wn, nn, ng):
    torus = Mesh(mesh.devices.reshape(nz, 2, ny, nx), ("z", "c", "y", "x"))
    SP, TP = ("z", "c"), ("y", "x")
    return jax.shard_map(
        functools.partial(local, (nz, ny, nx, tok, lat, d, wn, nn, ng)),
        mesh=torus,
        in_specs=(
            P(SP, TP),
            P(SP, TP),
            P(SP, None),
            P(SP, None),
            P(),
            P(None, TP),
            P(None, TP),
            P(TP, None),
            P(TP, None),
            P(SP, None),
            P(),
            P(SP, None),
            P(SP, None),
            P(SP, None, TP),
            P(SP, None, TP),
            P(SP, TP, None),
            P(None, TP),
            P(None, TP),
            P(TP, None),
        ),
        out_specs=P(SP, TP),
        check_vma=False,
    )


def solution(mesh):
    return build(mesh, 16, 4, 4, 64, 512, 2048, 128, 64, 4)
```

```python
import functools

import jax
import jax.numpy as jnp
import numpy as np
from jax import lax
from jax.experimental import pallas as pl
from jax.experimental.pallas import tpu as pltpu
from jax.sharding import Mesh
from jax.sharding import PartitionSpec as P

MESH = pl.DeviceIdType.MESH
ROPE = 32
CAP = 3
SLOTS = 8
THETA = 10000.0
EPS = 1e-06
FLOOR = -1e30
BF = jnp.bfloat16
F32 = jnp.float32


def rotary_table(tokens):
    half = ROPE // 2
    freq = np.float32(THETA) ** (-2.0 * np.arange(half, dtype=np.float32) / np.float32(ROPE))
    freq = freq.astype(np.float32)
    angles = np.arange(tokens, dtype=np.float32)[:, None] * freq[None, :]
    cosine = np.cos(angles.astype(np.float64)).astype(np.float32)
    sine = np.sin(angles.astype(np.float64)).astype(np.float32)
    return np.concatenate([cosine, cosine, -sine, sine], axis=1)


def dot(a, b, ca=1, cb=0):
    return lax.dot_general(a, b, (((ca,), (cb,)), ((), ())), preferred_element_type=F32)


def turned(values, table):
    half = ROPE // 2
    v = values.astype(F32)
    swapped = jnp.concatenate([v[:, half:], v[:, :half]], axis=1)
    return v * table[:, :ROPE] + swapped * table[:, ROPE : 2 * ROPE]


def normalized(values, gain):
    v = values.astype(F32)
    scaled = v * lax.rsqrt(jnp.mean(v * v, axis=-1, keepdims=True) + EPS)
    return (scaled * gain).astype(BF)


def eye(n):
    return lax.broadcasted_iota(jnp.int32, (n, n), 0) == lax.broadcasted_iota(jnp.int32, (n, n), 1)


def upright(line):
    return jnp.sum(jnp.where(eye(line.shape[1]), line, 0.0), axis=1, keepdims=True)


def silu(v):
    return v / (1.0 + jnp.exp(-v))


def shift_of(n):
    return n.bit_length() - 1


def kernel(dims, *refs):
    NZ, NY, NX, TOK, LAT, D, WN, NN, NG = dims
    NT, NS = NY * NX, NZ * 2
    LT, LC, DC = TOK // NY, LAT // NX, D // NT
    GZ = NZ // NG
    CH = GZ * LT
    KB = NY * CH
    HS = NS // NG
    Q = NS * SLOTS
    HQ = HS * SLOTS
    RPE = CAP * HS
    ROWS = 2 * RPE
    hbm, out_ref, scratch = refs[:20], refs[20], refs[21:]
    (
        v_wq, v_nq, v_lat, v_rk, v_lg, v_wkv, v_nkv, v_wno, v_res, v_ng, v_ids, v_rw,
        v_egu, v_ed, v_sgu, v_sd, v_tab,
        latn, rott, zbuf, zrot, lat_buf, rot_buf, qlat, qrp, mixd,
        pp, rsb, strm, sall, spp, shb, selt, disp, arr, xsend, xall, part, rs2, ret, back, v_wt,
        lsem, ss, rs, zsem, zsend, rsend, psem, psend, qsem, csem, csend, dsem, dsend, tsem, tsend, asem, xsem, esem,
    ) = scratch
    FF = v_sd.shape[0]
    WV, NV = hbm[7].shape[0], hbm[8].shape[0]
    vmem = [
        v_wq, v_nq, v_lat, v_rk, v_lg, v_wkv, v_nkv, v_wno.at[pl.ds(0, WV)], v_wno.at[pl.ds(WV, NV)],
        v_res, v_ng, v_ids, v_rw,
        v_egu.at[0], v_egu.at[1], v_ed,
        v_sgu.at[pl.ds(0, FF)], v_sgu.at[pl.ds(FF, FF)], v_sd, v_tab,
    ]

    z, c = lax.axis_index("z"), lax.axis_index("c")
    y, x = lax.axis_index("y"), lax.axis_index("x")
    t = y * NX + x
    s = z * 2 + c
    gz = lax.div(z, GZ)

    def plane(k):
        t2 = lax.rem(t + k, NT)
        return {"y": lax.div(t2, NX), "x": lax.rem(t2, NX)}, t2

    def seq(k):
        s2 = lax.rem(s + k + NS // 4, NS)
        return {"z": lax.div(s2, 2), "c": lax.rem(s2, 2)}, s2

    def others(f):
        each(0, NS - NS // 4, f)
        each(NS - NS // 4 + 1, NS, f)

    def cols(i):
        return pl.ds(pl.multiple_of(i * DC, DC), DC)

    def send(src, dst, ssem, rsem, dev):
        pltpu.make_async_remote_copy(
            src_ref=src, dst_ref=dst, send_sem=ssem, recv_sem=rsem, device_id=dev, device_id_type=MESH
        ).start()

    def keep(src, dst, sem):
        pltpu.make_async_copy(src, dst, sem).start()

    def wait(ref, sem, name="w"):
        with jax.named_scope(name):
            pltpu.make_async_copy(ref, ref, sem).wait()

    def each(lo, hi, f):
        run = 1
        if isinstance(lo, int) and isinstance(hi, int):
            run = max([u for u in range(1, 8) if (hi - lo) % u == 0], default=1)

        def body(k, carry):
            for i in range(run):
                f(lo + k * run + i if run > 1 else k)
            return carry

        if run > 1:
            lax.fori_loop(0, (hi - lo) // run, body, 0)
        else:
            lax.fori_loop(lo, hi, body, 0)

    bar = pltpu.get_barrier_semaphore()
    others(lambda k: pl.semaphore_signal(bar, inc=1, device_id=seq(k)[0], device_id_type=MESH))
    each(1, NT, lambda k: pl.semaphore_signal(bar, inc=1, device_id=plane(k)[0], device_id_type=MESH))

    loads = []
    for i in range(20):
        src = hbm[i]
        if i == 9:
            src = src.at[:, cols(t)]
        if i == 19:
            src = src.at[pl.ds(pl.multiple_of(s * TOK, TOK), TOK)]
        loads.append(pltpu.make_async_copy(src, vmem[i], lsem.at[i]))
    for i in (2, 3, 4, 19, 0, 1, 5, 6, 11, 12, 9, 7, 8, 10, 16, 17, 18, 13, 14, 15):
        loads[i].start()

    def loaded(*which):
        for i in which:
            loads[i].wait()

    def clear_tile(i):
        zbuf[gz, pl.ds(pl.multiple_of(i * LT, LT), LT)] = jnp.zeros((LT, LC), BF)

    def clear_turn(i):
        rot_buf[c, pl.ds(pl.multiple_of(i * LT, LT), LT)] = jnp.zeros((LT, ROPE * NY), BF)

    each(lax.rem(z, GZ) + 1, GZ, clear_tile)
    each(z + 1, NZ, clear_turn)

    loaded(2, 3, 4, 19)
    table = v_tab[...]
    latn[...] = normalized(v_lat[...], v_lg[...])
    rk = turned(dot(v_rk[...], eye(ROPE).astype(BF), 0, 0), table)
    rott[...] = jnp.concatenate([rk[i * LT : (i + 1) * LT] for i in range(NY)], axis=1).astype(BF)

    with jax.named_scope("w_bar"):
        pl.semaphore_wait(bar, NS + NT - 2)

    own_tile = latn.at[pl.ds(pl.multiple_of(y * LT, LT), LT), pl.ds(pl.multiple_of(x * LC, LC), LC)]
    zslot = zbuf.at[gz, pl.ds(pl.multiple_of(lax.rem(z, GZ) * LT, LT), LT)]

    each(1, NZ - z, lambda k: send(own_tile, zslot, zsend.at[k], zsem.at[z], {"z": NZ - k}))
    keep(own_tile, zslot, zsem.at[z])

    @pl.when(z == t)
    def _():
        each(1, NZ - z, lambda k: send(rott, zrot, rsend.at[k], rs.at[1], {"z": z + k}))
        keep(rott, zrot, rs.at[1])

    loaded(0, 1, 5, 6)
    wscale, nscale = (WN + ROPE) ** -0.5, (NN + ROPE) ** -0.5
    qlat[:TOK] = (dot(v_wq[:, :WN], v_wkv[:, :WN], 1, 1) * wscale).astype(BF)
    qlat[TOK:] = (dot(v_nq[:, :NN], v_nkv[:, :NN], 1, 1) * nscale).astype(BF)
    qr = jnp.concatenate(
        [turned(v_wq[:, WN:], table) * wscale, turned(v_nq[:, NN:], table) * nscale], axis=0
    )
    qrp[...] = jnp.concatenate([qr] * NY, axis=1).astype(BF)

    def lat_slot(g):
        return lat_buf.at[c, g, y, :, x_cols]

    x_cols = pl.ds(pl.multiple_of(x * LC, LC), LC)
    HC = CH // 2
    half = (pl.ds(0, HC), pl.ds(HC, HC))
    two = lax.div(gz, NG - 1)

    def along_x(f):
        each(1, NX, lambda k: f({"x": lax.rem(x + k, NX)}))

    def along_y(f):
        each(1, NY, lambda k: f({"y": lax.rem(y + k, NY)}))

    def group_on(k):
        g = group(k)
        row = lat_buf.at[c, g, y, half[0], :]
        wait(row, tsem.at[0, g], "w_step")
        along_y(lambda dev: send(row, row, tsend.at[2, g], tsem.at[2, g], dev))
        column = lat_buf.at[c, g, :, half[1], x_cols]
        wait(column, tsem.at[1, g], "w_step")
        along_x(lambda dev: send(column, column, tsend.at[3, g], tsem.at[3, g], dev))

    wrap = lax.div(z, NZ - 2) if NG > 2 else 0

    def group(k):
        first = lax.div(NG - k, NG)
        second = lax.div(NG + 1 - k, NG) - first
        top = lax.div(gz, NG - 1)
        near = lax.div(NG + 2 - k, NG) - first
        far_last = first * gz + near * (NG - 2) * (second * (1 - wrap) + (1 - second) * wrap) + (1 - first - near) * 1
        return top * far_last + (1 - top) * (gz - k) if NG > 2 else gz - k

    my_rot = rot_buf.at[c, pl.ds(pl.multiple_of(t * LT, LT), LT)]

    def tiles_of(g, k):
        lo = g * GZ
        whole = 1 - lax.div(NG - k, NG)
        return lo, lo + whole * GZ + (1 - whole) * (lax.rem(z, GZ) + 1)

    def group_out(k):
        g = group(k)
        each(*tiles_of(g, k), lambda i: wait(zslot, zsem.at[i], "w_z"))

        @pl.when((lax.div(t, GZ) == g) & (t <= z))
        def _():
            wait(zrot, rs.at[1], "w_zrot")
            keep(zrot, my_rot, qsem.at[t])
            each(1, NT, lambda i: send(zrot, my_rot, ss.at[3], qsem.at[t], plane(i)[0]))

        @pl.when(two == 0)
        def _():
            keep(zbuf.at[g], lat_slot(g), psem.at[g])
            each(1, NT, lambda i: send(zbuf.at[g], lat_slot(g), psend.at[g], psem.at[g], plane(i)[0]))

        @pl.when(two == 1)
        def _():
            for i, along in ((0, along_x), (1, along_y)):
                src, dst = zbuf.at[g, half[i]], lat_buf.at[c, g, y, half[i], x_cols]
                keep(src, dst, tsem.at[i, g])
                along(lambda dev, src=src, dst=dst, i=i: send(src, dst, tsend.at[i, g], tsem.at[i, g], dev))

    each(0, 1, group_out)

    @pl.when(two == 1)
    def _():
        each(0, 1, group_on)

    each(1, gz + 1, group_out)

    @pl.when(two == 1)
    def _():
        each(1, gz + 1, group_on)

    loaded(11, 12)
    lane = lax.broadcasted_iota(jnp.int32, (TOK, Q), 1)
    j = lane & (SLOTS - 1)
    high = (j >= CAP).astype(jnp.int32)
    expert = ((lane >> shift_of(SLOTS)) * 2 + high).astype(F32)
    hit0 = upright(v_ids[0:1].astype(F32)) == expert
    hit1 = upright(v_ids[1:2].astype(F32)) == expert
    ahead = (
        lax.broadcasted_iota(jnp.int32, (TOK, TOK), 0) > lax.broadcasted_iota(jnp.int32, (TOK, TOK), 1)
    ).astype(F32)
    hits = jnp.where(hit0 | hit1, 1.0, 0.0).astype(F32)
    rank = dot(ahead.astype(BF), hits.astype(BF))
    fits = (rank == (j - CAP * high).astype(F32)) & (j < 2 * CAP)
    selt[0] = jnp.where(hit0 & fits, 1.0, 0.0).astype(BF)
    selt[1] = jnp.where(hit1 & fits, 1.0, 0.0).astype(BF)

    other = {"c": 1 - c}

    def turn_rows(p, g):
        return rot_buf.at[p, pl.ds(pl.multiple_of(g * CH, CH), CH)]

    def group_over(k):
        g = group(k)

        @pl.when(two == 0)
        def _():
            wait(lat_buf.at[c, g], psem.at[g], "w_plane")

        @pl.when(two == 1)
        def _():
            wait(lat_buf.at[c, g, pl.ds(0, NY - 1), half[0], :], tsem.at[2, g], "w_plane")
            wait(lat_buf.at[c, g, :, half[1], pl.ds(0, (NX - 1) * LC)], tsem.at[3, g], "w_plane")

        send(lat_buf.at[c, g], lat_buf.at[c, g], csend.at[g], csem.at[g], other)
        each(*tiles_of(g, k), lambda i: wait(zrot, qsem.at[i], "w_prot"))
        send(turn_rows(c, g), turn_rows(c, g), dsend.at[g], dsem.at[g], other)

    key = lax.broadcasted_iota(jnp.int32, (2 * TOK, KB), 1)
    key_at = (
        (key >> shift_of(CH)) * LT + ((key >> shift_of(LT)) & (GZ - 1)) * (2 * TOK) + (key & (LT - 1))
    )
    query_at = s * TOK + (lax.broadcasted_iota(jnp.int32, (2 * TOK, KB), 0) & (TOK - 1))
    ahead_by = query_at - key_at
    strip = lax.broadcasted_iota(jnp.int32, (CH, ROPE * NY), 1) >> shift_of(ROPE)
    mixd[...] = jnp.zeros_like(mixd)

    def scored(p, g):
        turns = rot_buf[p, pl.ds(pl.multiple_of(g * CH, CH), CH)].astype(F32)
        turns = jnp.concatenate([jnp.where(strip == i, turns, 0.0) for i in range(NY)], axis=0)
        keys = lat_buf[p, g].reshape(KB, LAT)
        scores = dot(qlat[...], keys, 1, 1) + dot(qrp[...], turns.astype(BF), 1, 1)
        return jnp.where(ahead_by >= p * TOK + g * (GZ * 2 * TOK), scores, FLOOR)

    def attend(places, carry):
        peak, total = carry
        scores = [scored(p, g) for p, g in places]
        newest = peak
        for sc in scores:
            newest = jnp.maximum(newest, jnp.max(sc, axis=-1, keepdims=True))
        fade = jnp.exp(peak - newest)
        mixed, total = mixd[...] * fade, total * fade
        for (p, g), sc in zip(places, scores):
            probs = jnp.exp(sc - newest)
            total = total + jnp.sum(probs, axis=-1, keepdims=True)
            mixed = mixed + dot(probs.astype(BF), lat_buf[p, g].reshape(KB, LAT))
        mixd[...] = mixed
        return newest, total

    def wait_other(k):
        g = group(k)
        wait(lat_buf.at[1 - c, g], csem.at[g], "w_core")
        wait(turn_rows(1 - c, g), dsem.at[g], "w_crot")

    def both_attend(k, carry):
        group_over(k)
        wait_other(k - 1)
        return attend([(c, group(k)), (1 - c, group(k - 1))], carry)

    carry = (jnp.full((2 * TOK, 1), FLOOR, F32), jnp.zeros((2 * TOK, 1), F32))
    group_over(0)
    carry = attend([(c, gz)], carry)
    carry = lax.fori_loop(1, gz + 1, both_attend, carry)
    wait_other(gz)
    _, total = attend([(1 - c, group(gz))], carry)
    mixed = (mixd[...] / total).astype(BF)
    wide = dot(mixed[:TOK], v_wkv[:, WN:])
    narrow = dot(mixed[TOK:], v_nkv[...])[:, NN:]
    loaded(7, 8, 9)
    pp[...] = dot(jnp.concatenate([wide, narrow], axis=1).astype(BF), v_wno[...]).astype(BF)

    late = z >= GZ

    def spread(rows, slots, r_axis):
        row = lax.broadcasted_iota(jnp.int32, (rows, slots), r_axis)
        slot = lax.broadcasted_iota(jnp.int32, (rows, slots), 1 - r_axis)
        return jnp.where(slot == (row & (HS - 1)) * SLOTS + (row >> shift_of(HS)), 1.0, 0.0).astype(BF)

    def rows_out(h):
        wait(arr.at[pl.ds(h * HS, HS)], asem.at[h], f"w_arr{h}")
        came = arr[h * HS : (h + 1) * HS].astype(F32).reshape(HQ, DC).astype(BF)
        xsend[h] = dot(spread(ROWS, HQ, 0), came).astype(BF)
        each(1, NT, lambda k: send(xsend.at[h], xall.at[h, :, cols(t)], ss.at[10], xsem.at[h], plane(k)[0]))
        keep(xsend.at[h], xall.at[h, :, cols(t)], xsem.at[h])

    def experts(h):
        wait(xall.at[h], xsem.at[h], f"w_xall{h}")
        both = dot(normalized(xall[h], v_ng[...]), v_wt[...])
        hidden = silu(both[:, : 2 * FF]) * both[:, 2 * FF :]
        first = lax.broadcasted_iota(jnp.int32, (ROWS, 2 * FF), 0) < RPE
        hidden = jnp.where(first == (lax.broadcasted_iota(jnp.int32, (ROWS, 2 * FF), 1) < FF), hidden, 0.0)
        part[h] = dot(hidden.astype(BF), v_ed[...].reshape(2 * FF, D)).astype(BF)

        def e_send(k):
            dev, t2 = plane(k)
            send(part.at[h, :, cols(t2)], rs2.at[h, k - 1], ss.at[11], esem.at[h], dev)

        each(1, NT, e_send)

    def rows_back(h):
        acc = part[h, :, cols(t)].astype(F32)
        wait(rs2.at[h], esem.at[h], f"w_rs2_{h}")
        for k in range(NT - 1):
            acc = acc + rs2[h, k].astype(F32)
        ret[h] = dot(spread(HQ, ROWS, 1), acc.astype(BF)).reshape(HS, SLOTS, DC).astype(BF)

        def b_send(k):
            r2 = lax.rem(s + k, HS)
            s2 = h * HS + r2

            @pl.when(s2 != s)
            def _():
                send(ret.at[h, r2], back.at[s], ss.at[12], rs.at[11], {"z": lax.div(s2, 2), "c": lax.rem(s2, 2)})

            @pl.when(s2 == s)
            def _():
                keep(ret.at[h, r2], back.at[s], rs.at[11])

        each(0, HS, b_send)

    def pp_send(k):
        dev, t2 = plane(k)
        send(pp.at[:, cols(t2)], rsb.at[k - 1], ss.at[6], rs.at[5], dev)

    each(1, NT, pp_send)
    loaded(10, 16, 17, 18, 13, 14, 15)
    v_wt[...] = v_egu[...].reshape(4 * FF, D).T
    acc = pp[:, cols(t)].astype(F32)
    wait(rsb, rs.at[5], "w_proj")
    for k in range(NT - 1):
        acc = acc + rsb[k].astype(F32)
    stream = (v_res[...].astype(F32) + acc.astype(BF).astype(F32)).astype(BF)
    strm[...] = stream

    bunch = lax.div(s, HS)
    disp[...] = dot(selt[0] + selt[1], stream, 0, 0).reshape(NS, SLOTS, DC).astype(BF)

    def d_send(k):
        dev, s2 = seq(k)
        send(disp.at[s2], arr.at[s], ss.at[7], asem.at[bunch], dev)

    others(d_send)
    keep(disp.at[s], arr.at[s], asem.at[bunch])

    def stream_out():
        each(1, NT, lambda k: send(strm, sall.at[:, cols(t)], ss.at[8], rs.at[7], plane(k)[0]))
        keep(strm, sall.at[:, cols(t)], rs.at[7])

    def shared_expert():
        wait(sall, rs.at[7], "w_sall")
        both = dot(normalized(sall[...], v_ng[...]), v_sgu[...], 1, 1)
        hidden = (silu(both[:, :FF]) * both[:, FF:]).astype(BF)
        spp[...] = dot(hidden, v_sd[...]).astype(BF)

    def shared_out():
        def sh_send(k):
            dev, t2 = plane(k)
            send(spp.at[:, cols(t2)], shb.at[k - 1], ss.at[9], rs.at[8], dev)

        each(1, NT, sh_send)

    @pl.when(jnp.logical_not(late))
    def _():
        stream_out()
        rows_out(0)
        shared_expert()
        shared_out()

    @pl.when(late)
    def _():
        rows_out(0)
        stream_out()

    rows_out(1)
    experts(0)
    for h in range(2, NG):
        rows_out(h)
    for h in range(1, NG - 1):
        experts(h)
        if h == 1:
            rows_back(0)
    experts(NG - 1)
    for h in range(1 if NG > 2 else 0, NG - 1):
        rows_back(h)

    @pl.when(late)
    def _():
        shared_expert()
        shared_out()

    rows_back(NG - 1)

    each(1, NZ - z, lambda k: wait(zslot, zsend.at[k]))

    @pl.when(z == t)
    def _():
        each(1, NZ - z, lambda k: wait(zrot, rsend.at[k]))

    chunks = rsb if CH * LC == TOK * DC else lat_buf.at[0, 0, :, pl.ds(0, CH * (NT - 1) // NT)]

    @pl.when(two == 0)
    def _():
        each(0, gz + 1, lambda g: wait(chunks, psend.at[g]))

    @pl.when(two == 1)
    def _():
        def left(g):
            wait(lat_buf.at[0, 0, 0, half[0], pl.ds(0, (NX - 1) * LC)], tsend.at[0, g])
            wait(lat_buf.at[0, 0, pl.ds(0, NY - 1), half[0], pl.ds(0, LC)], tsend.at[1, g])
            wait(lat_buf.at[0, 0, pl.ds(0, NY - 1), half[0], :], tsend.at[2, g])
            wait(lat_buf.at[0, 0, :, half[0], pl.ds(0, (NX - 1) * LC)], tsend.at[3, g])

        each(0, gz + 1, left)

    @pl.when(t <= z)
    def _():
        wait(rot_buf.at[0, pl.ds(0, (NT - 1) * LT)], ss.at[3])

    each(0, gz + 1, lambda g: wait(lat_buf.at[0, 0], csend.at[g]))
    each(0, gz + 1, lambda g: wait(turn_rows(0, 0), dsend.at[g]))
    wait(rsb, ss.at[6])
    wait(disp.at[pl.ds(0, NS - 1)], ss.at[7])
    wait(rsb, ss.at[8])
    wait(rs2, ss.at[10])
    wait(rs2, ss.at[11])

    first_weight, second_weight = upright(v_rw[0:1]), upright(v_rw[1:2])
    shared = spp[:, cols(t)].astype(F32)
    wait(shb, rs.at[8], "w_shb")
    for k in range(NT - 1):
        shared = shared + shb[k].astype(F32)
    before = strm[...].astype(F32) + shared.astype(BF).astype(F32)

    wait(back, rs.at[11], "w_back")
    rows = back[...].astype(F32).reshape(Q, DC).astype(BF)
    picked = dot(selt[...].reshape(2 * TOK, Q), rows)
    routed = picked[:TOK] * first_weight + picked[TOK:] * second_weight
    out_ref[...] = (before + routed).astype(BF)
    wait(shb, ss.at[9])
    wait(back.at[pl.ds(0, NS - 1)], ss.at[12])


def local(dims, *args):
    NZ, NY, NX, TOK, LAT, D, WN, NN, NG = dims
    NT, NS = NY * NX, NZ * 2
    LT, LC, DC = TOK // NY, LAT // NX, D // NT
    CH = NZ // NG * LT
    HS = NS // NG
    ROWS = 2 * CAP * HS
    args = list(args)
    args[4] = args[4].reshape(1, -1)
    args[10] = args[10].reshape(1, -1)
    for i in (3, 11, 12, 13, 14, 16, 17):
        args[i] = jnp.swapaxes(args[i], -1, -2)
    FF = args[18].shape[0]
    args.append(jnp.asarray(rotary_table(NS * TOK)))
    shapes = [a.shape for a in args]
    shapes[9] = (TOK, DC)
    shapes[19] = (TOK, 2 * ROPE)
    shapes[13] = (2, 2, FF, D)
    shapes[16] = (2 * FF, D)
    shapes[7] = (shapes[7][0] + shapes[8][0], D)
    kept = [i for i in range(20) if i not in (8, 14, 17)]
    scratch = [pltpu.VMEM(shapes[i], args[i].dtype) for i in kept]
    scratch += [
        pltpu.VMEM((TOK, LAT), BF),
        pltpu.VMEM((LT, ROPE * NY), BF),
        pltpu.VMEM((NG, CH, LC), BF),
        pltpu.VMEM((LT, ROPE * NY), BF),
        pltpu.VMEM((2, NG, NY, CH, LAT), BF),
        pltpu.VMEM((2, NZ * LT, ROPE * NY), BF),
        pltpu.VMEM((2 * TOK, LAT), BF),
        pltpu.VMEM((2 * TOK, ROPE * NY), BF),
        pltpu.VMEM((2 * TOK, LAT), F32),
        pltpu.VMEM((TOK, D), BF),
        pltpu.VMEM((NT - 1, TOK, DC), BF),
        pltpu.VMEM((TOK, DC), BF),
        pltpu.VMEM((TOK, D), BF),
        pltpu.VMEM((TOK, D), BF),
        pltpu.VMEM((NT - 1, TOK, DC), BF),
        pltpu.VMEM((2, TOK, NS * SLOTS), BF),
        pltpu.VMEM((NS, SLOTS, DC), BF),
        pltpu.VMEM((NS, SLOTS, DC), BF),
        pltpu.VMEM((NG, ROWS, DC), BF),
        pltpu.VMEM((NG, ROWS, D), BF),
        pltpu.VMEM((NG, ROWS, D), BF),
        pltpu.VMEM((NG, NT - 1, ROWS, DC), BF),
        pltpu.VMEM((NG, HS, SLOTS, DC), BF),
        pltpu.VMEM((NS, SLOTS, DC), BF),
        pltpu.VMEM((D, 4 * FF), BF),
        pltpu.SemaphoreType.DMA((20,)),
        pltpu.SemaphoreType.DMA((13,)),
        pltpu.SemaphoreType.DMA((12,)),
        pltpu.SemaphoreType.DMA((NZ,)),
        pltpu.SemaphoreType.DMA((NZ,)),
        pltpu.SemaphoreType.DMA((NZ,)),
        pltpu.SemaphoreType.DMA((NG,)),
        pltpu.SemaphoreType.DMA((NG,)),
        pltpu.SemaphoreType.DMA((NT,)),
        pltpu.SemaphoreType.DMA((NG,)),
        pltpu.SemaphoreType.DMA((NG,)),
        pltpu.SemaphoreType.DMA((NG,)),
        pltpu.SemaphoreType.DMA((NG,)),
        pltpu.SemaphoreType.DMA((4, NG)),
        pltpu.SemaphoreType.DMA((4, NG)),
        pltpu.SemaphoreType.DMA((NG,)),
        pltpu.SemaphoreType.DMA((NG,)),
        pltpu.SemaphoreType.DMA((NG,)),
    ]
    return pl.pallas_call(
        functools.partial(kernel, dims),
        out_shape=pltpu.VMEM((TOK, DC), BF),
        in_specs=[pl.BlockSpec(memory_space=pltpu.HBM)] * 20,
        out_specs=pl.BlockSpec(memory_space=pltpu.VMEM),
        scratch_shapes=scratch,
        compiler_params=pltpu.CompilerParams(
            collective_id=0, has_side_effects=True, vmem_limit_bytes=60 * 1024 * 1024
        ),
        name="layer",
    )(*args)


def build(mesh, nz, ny, nx, tok, lat, d, wn, nn, ng):
    torus = Mesh(mesh.devices.reshape(nz, 2, ny, nx), ("z", "c", "y", "x"))
    SP, TP = ("z", "c"), ("y", "x")
    return jax.shard_map(
        functools.partial(local, (nz, ny, nx, tok, lat, d, wn, nn, ng)),
        mesh=torus,
        in_specs=(
            P(SP, TP),
            P(SP, TP),
            P(SP, None),
            P(SP, None),
            P(),
            P(None, TP),
            P(None, TP),
            P(TP, None),
            P(TP, None),
            P(SP, None),
            P(),
            P(SP, None),
            P(SP, None),
            P(SP, None, TP),
            P(SP, None, TP),
            P(SP, TP, None),
            P(None, TP),
            P(None, TP),
            P(TP, None),
        ),
        out_specs=P(SP, TP),
        check_vma=False,
    )


def solution(mesh):
    return build(mesh, 16, 4, 4, 64, 512, 2048, 128, 64, 4)
```
